32 devices in a mesh: ep: 8 (over z, y), tp: 4 (over x, core).
Axes of the slice: x: 2, y: 2, z: 4, core: 2. Of those that a mesh axis runs over, the one named last changes fastest.
Arguments:
- queries: bfloat16 [4096, 1024], P('ep', 'tp'), may hold values from -6 to 6
- keys: bfloat16 [4096, 512], P('ep', 'tp'), may hold values from -6 to 6
- values: bfloat16 [4096, 512], P('ep', 'tp'), may hold values from -6 to 6
- forget_cache: float32 [8, 4096], P('tp'), may hold values from -412 to 0, as said below
- query_gain: float32 [128], replicated, may hold values from 0.6 to 6
- key_gain: float32 [128], replicated, may hold values from 0.6 to 6
- mixer_out: bfloat16 [1024, 2048], replicated, may hold values from -0.75 to 0.75
- expert_input: bfloat16 [4096, 2048], P(('ep', 'tp')), may hold values from -6 to 6
- norm_gain: float32 [2048], replicated, may hold values from 0.1 to 1.9
- routes: int32 [4096, 2], P(('ep', 'tp')), may hold values from 0 to 31, all different within a row; in each aligned block of 128 rows (0 to 127, 128 to 255, ...) at most 16 rows name the same one
- route_weights: float32 [4096, 2], P(('ep', 'tp')), may hold values from 0.1 to 1
- w_gate: bfloat16 [32, 2048, 1024], P('ep', None, 'tp'), may hold values from -0.125 to 0.125
- w_up: bfloat16 [32, 2048, 1024], P('ep', None, 'tp'), may hold values from -0.125 to 0.125
- w_down: bfloat16 [32, 2048, 1024], P('ep', None, 'tp'), may hold values from -0.1875 to 0.1875
Outputs:
- mixed: bfloat16 [4096, 2048], P(('ep', 'tp'))
- routed: bfloat16 [4096, 2048], P(('ep', 'tp'))
The draws below stay inside these ranges and needn't reach their ends.
Inputs may be any that keep to these rules, and one draw needn't show every extreme that they name: `routes`: each row names 2 different experts; among the rows of one device no expert is named by more than 16 rows, a bound that some block reaches. `forget_cache`: never rises along the positions.
All inputs are finite; a program needn't handle non-finite values.
Results may differ from the reference program's by a relative error of at most 0.013.
The reference program's roundings to bfloat16 on the way count: a program that leaves them out, or rounds other values in their place, can miss the bound.
Values may be sent and summed in bfloat16 or wider, within the bound.
A program may use at most 128 MiB of HBM per device.

```python
import math
import jax
import jax.numpy as jnp
import numpy as np
from jax import lax

D = 2048
QUERY_HEADS = 8
KV_HEADS = 4
HD = 128
EXPERTS = 32
TOPK = 2
FF = 1024
TB_DEV = 128
CAP = 16
ATTENTION_TOKENS = 4096
TOK_B = 4096
N_EP = 8
N_TP = 4


def draw_forget_cache(key, part):
    parallel_flows = jax.random.split(jax.random.fold_in(key, 11), 5)
    token_positions = jnp.arange(ATTENTION_TOKENS, dtype=jnp.int32)
    order = jax.random.permutation(parallel_flows[0], QUERY_HEADS)
    quick = order < QUERY_HEADS // 2
    rate = jnp.where(quick, 1.0 / 40.0, 0.8 / ATTENTION_TOKENS)
    rough = jax.random.uniform(parallel_flows[1], (QUERY_HEADS, ATTENTION_TOKENS), jnp.float32, 0.3, 1.7)
    blocks = 16
    factor = jnp.exp(jax.random.uniform(parallel_flows[2], (QUERY_HEADS, blocks), jnp.float32, -0.7, 0.7))
    which = token_positions * blocks // ATTENTION_TOKENS
    steps = -rate[:, None] * rough * factor[:, which]
    token_groups = jax.random.randint(parallel_flows[3], (QUERY_HEADS, 3), 0, ATTENTION_TOKENS)
    depth = jnp.log(jax.random.uniform(parallel_flows[4], (QUERY_HEADS, 3), jnp.float32, 0.5, 0.8))
    masked_scores = token_positions[None, None, :] == token_groups[:, :, None]
    steps = steps + jnp.sum(jnp.where(masked_scores, depth[:, :, None], 0.0), axis=1)
    return jnp.cumsum(steps, axis=1).astype(jnp.float32)


def draw_query_gain(key, part):
    return jax.random.uniform(jax.random.fold_in(key, 21), (HD,), jnp.float32, 0.6, 1.4)


def draw_key_gain(key, part):
    return jax.random.uniform(jax.random.fold_in(key, 31), (HD,), jnp.float32, 0.6, 1.4)


def block_scale(own_key, shape, cuts, low, largest):
    factor_of = 1.0
    for position, blocks in cuts:
        steps = jax.random.uniform(jax.random.fold_in(jax.random.fold_in(own_key, 6), position), (blocks,), jnp.float32, low / len(cuts), largest / len(cuts))
        factor_of = factor_of * jnp.repeat(jnp.exp(steps), shape[position] // blocks).reshape((-1,) + (1,) * (len(shape) - 1 - position))
    return factor_of


def routed_block(key, own, number, rows, amount, top, most, lean):
    ranking = jax.random.permutation(key, amount)
    crowded, usual = portions_of(amount, rows * top, most, lean, True), portions_of(amount, rows * top, most, lean, False)
    places = jnp.arange(amount)

    def named(tallies, rotation):
        used = int((tallies > 0).sum())
        fixed = max(1, used // 4)
        passed = fixed + (places - fixed + rotation * (used - fixed)) % max(1, amount - fixed)
        return jnp.zeros((amount,), jnp.int32).at[ranking[jnp.where(places < fixed, places, passed)]].set(jnp.asarray(tallies, jnp.int32))

    tallies = jnp.where(number % 4 == 0, named(crowded, number // 4), named(usual, number - number // 4 - 1))
    mixed = jax.random.permutation(jax.random.fold_in(own, 3), amount)
    giver, sink = mixed[0:amount // 2 * 2:2], mixed[1:amount // 2 * 2:2]
    margin = jnp.minimum(tallies[giver] - 1, most - tallies[sink]) // 2
    margin = jnp.where((giver == ranking[0]) | (sink == ranking[0]) | (tallies[sink] == 0), 0, jnp.maximum(margin, 0))
    passed = jax.random.randint(jax.random.fold_in(own, 4), (amount // 2,), 0, 1 << 20) % (margin + 1)
    tallies = tallies.at[giver].add(-passed).at[sink].add(passed)
    items = jnp.searchsorted(jnp.cumsum(tallies), jnp.arange(rows * top), side="right").astype(jnp.int32)
    grid = items.reshape(top, rows).T
    grid = grid[jax.random.permutation(jax.random.fold_in(own, 1), rows)]
    rotation = jax.random.randint(jax.random.fold_in(own, 2), (rows, 1), 0, top)
    return jnp.take_along_axis(grid, (jnp.arange(top)[None, :] + rotation) % top, axis=1)


def portions_of(number_of, total, limit, slope, full):
    loads = [(1 << 20) // math.isqrt(rank ** slope) + 1 for rank in range(1, number_of + 1)]
    largest = limit if full else min(limit, max(-(-total // number_of), total * loads[0] // sum(loads)))
    least = 1 if total - largest >= number_of - 1 else 0
    holding, spare = [largest] + [least] * (number_of - 1), total - largest - least * (number_of - 1)
    while spare > 0:
        free = [i for i in range(1, number_of) if holding[i] < largest] or [i for i in range(1, number_of) if holding[i] < limit]
        pool, left = sum([loads[i] for i in free]), spare
        for i in free:
            addition = min(limit - holding[i], max(1, left * loads[i] // pool), spare)
            holding[i] = holding[i] + addition
            spare = spare - addition
    return np.array(holding)


def scatter_about(rng, shape, deviation, limit, pieces=(), kind=jnp.bfloat16):
    drawn = deviation * jax.random.normal(rng, shape, jnp.float32)
    if pieces:
        drawn = drawn * block_scale(rng, shape, pieces, -0.22, 0.18)
    return jnp.clip(drawn, -limit, limit).astype(kind)


def setup_inputs(seed: int = 0) -> dict:
    streams_of = jax.random.split(jax.random.key(seed), 15)
    queries = scatter_about(streams_of[0], (ATTENTION_TOKENS, QUERY_HEADS * HD), 1.0, 6.0, ((0, 8), (1, 4)))
    keys = scatter_about(streams_of[1], (ATTENTION_TOKENS, KV_HEADS * HD), 1.0, 6.0, ((0, 8), (1, 4)))
    values = scatter_about(streams_of[2], (ATTENTION_TOKENS, KV_HEADS * HD), 1.0, 6.0, ((0, 8), (1, 4)))
    forget_cache = draw_forget_cache(jax.random.fold_in(streams_of[14], 71), 0)
    query_gain = draw_query_gain(jax.random.fold_in(streams_of[14], 71), 0)
    key_gain = draw_key_gain(jax.random.fold_in(streams_of[14], 71), 0)
    mixer_out = scatter_about(streams_of[6], (QUERY_HEADS * HD, D), (QUERY_HEADS * HD // 16) ** -0.5, 0.75)
    expert_input = scatter_about(streams_of[7], (TOK_B, D), 1.0, 6.0, ((0, 32),))
    norm_gain = jnp.clip(1.0 + 0.18 * jax.random.normal(streams_of[8], (D,), jnp.float32), 0.1, 1.9)
    routes_keys = jax.random.split(jax.random.fold_in(streams_of[9], 1), TOK_B // TB_DEV)
    routes_turns = jax.random.permutation(jax.random.fold_in(streams_of[9], 3), TOK_B // TB_DEV)
    routes = jax.vmap(lambda own, number: routed_block(jax.random.fold_in(streams_of[9], 2), own, number, TB_DEV, EXPERTS, TOPK, CAP, 1))(routes_keys, routes_turns).reshape((TOK_B, TOPK))
    route_weights = jnp.clip(0.1 + 0.9 * jax.random.uniform(streams_of[10], (TOK_B, TOPK), jnp.float32) ** block_scale(streams_of[10], (TOK_B, TOPK), ((0, 32),), -0.2, 0.2), 0.1, 1.0)
    w_gate = scatter_about(streams_of[11], (EXPERTS, D, FF), D ** -0.5, 0.125, ((0, 8), (2, 4)))
    w_up = scatter_about(streams_of[12], (EXPERTS, D, FF), D ** -0.5, 0.125, ((0, 8), (2, 4)))
    w_down = scatter_about(streams_of[13], (EXPERTS, D, FF), FF ** -0.5, 0.1875, ((0, 8), (2, 4)))
    return dict(queries=queries, keys=keys, values=values, forget_cache=forget_cache, query_gain=query_gain, key_gain=key_gain, mixer_out=mixer_out, expert_input=expert_input, norm_gain=norm_gain, routes=routes, route_weights=route_weights, w_gate=w_gate, w_up=w_up, w_down=w_down)


EPSILON = 1e-06
NEGATIVE = -1e+30

def rms_scale(inputs, gain):
    inputs = inputs.astype(jnp.float32)
    return inputs * lax.rsqrt(lax.optimization_barrier(jnp.mean(inputs * inputs, axis=-1, keepdims=True)) + EPSILON) * gain

def reference(queries, keys, values, forget_cache, query_gain, key_gain, mixer_out, expert_input, norm_gain, routes, route_weights, w_gate, w_up, w_down):
    total = queries.shape[0]
    group = QUERY_HEADS // KV_HEADS
    normed_q = rms_scale(queries.reshape(total, QUERY_HEADS, HD), query_gain).astype(jnp.bfloat16)
    normed_q = lax.optimization_barrier(normed_q).astype(jnp.float32)
    normed_k = rms_scale(keys.reshape(total, KV_HEADS, HD), key_gain).astype(jnp.bfloat16)
    normed_k = lax.optimization_barrier(normed_k).astype(jnp.float32)
    key_heads = jnp.repeat(normed_k, group, axis=1)
    value_heads = jnp.repeat(values.reshape(total, KV_HEADS, HD).astype(jnp.float32), group, axis=1)
    block = math.gcd(total, 512)
    token_positions = jnp.arange(total, dtype=jnp.int32)
    scale = HD ** (-0.5)

    def one_block(number):
        first = (number * block).astype(jnp.int32)
        query_block = lax.dynamic_slice_in_dim(normed_q, first, block, 0)
        scores = jnp.einsum('qhd,khd->hqk', query_block, key_heads) * scale
        gates_q = lax.dynamic_slice_in_dim(forget_cache, first, block, 1)
        scores = scores + gates_q[:, :, None] - forget_cache[:, None, :]
        allowed = token_positions[None, :] <= (first + jnp.arange(block, dtype=jnp.int32))[:, None]
        scores = jnp.where(allowed[None], scores, NEGATIVE)
        highest = lax.optimization_barrier(jnp.max(scores, axis=2, keepdims=True))
        weights = jnp.where(allowed[None], jnp.exp(scores - highest), 0.0)
        denom = lax.optimization_barrier(jnp.sum(weights, axis=2))
        rounded = lax.optimization_barrier(weights.astype(jnp.bfloat16)).astype(jnp.float32)
        numer = jnp.einsum('hqk,khd->qhd', rounded, value_heads)
        return (numer / denom.T[:, :, None]).astype(jnp.bfloat16)
    attended = lax.map(one_block, jnp.arange(total // block, dtype=jnp.int32)).reshape(total, QUERY_HEADS * HD)
    mixed = jnp.dot(attended, mixer_out, preferred_element_type=jnp.float32).astype(jnp.bfloat16)
    normed_b = rms_scale(expert_input, norm_gain).astype(jnp.bfloat16)
    count = expert_input.shape[0]
    flat = routes.reshape(-1)
    most = N_EP * N_TP * CAP
    padded = jnp.concatenate([normed_b, jnp.zeros((1, D), jnp.bfloat16)], axis=0)
    flat_weights = jnp.concatenate([route_weights.reshape(-1), jnp.zeros((1,), jnp.float32)])

    def per_expert(totals, expert):
        chosen = jnp.nonzero(flat == expert, size=most, fill_value=flat.shape[0])[0].astype(jnp.int32)
        owner = (chosen // TOPK).astype(jnp.int32)
        rows = padded[owner]
        gate = jnp.dot(rows, w_gate[expert], preferred_element_type=jnp.float32)
        upward = jnp.dot(rows, w_up[expert], preferred_element_type=jnp.float32)
        hidden = (jax.nn.silu(gate) * upward).astype(jnp.bfloat16)
        output = jnp.dot(hidden, w_down[expert].T, preferred_element_type=jnp.float32).astype(jnp.bfloat16)
        return (totals.at[owner].add(output.astype(jnp.float32) * flat_weights[chosen][:, None]), None)
    totals = lax.scan(per_expert, jnp.zeros((count + 1, D), jnp.float32), jnp.arange(EXPERTS, dtype=jnp.int32))[0]
    routed = totals[:count].astype(jnp.bfloat16)
    return (mixed, routed)
```

```python
import functools

import jax
import jax.numpy as jnp
from jax import lax
from jax.experimental import pallas as pl
from jax.experimental.pallas import tpu as pltpu
from jax.sharding import PartitionSpec as P

CAP = 16
EPSILON = 1e-06
NEGATIVE = -1e30
MESH = pl.DeviceIdType.MESH
VMEM_LIMIT = 62 * 1024 * 1024


def places(n_tp):
    ep, tp = lax.axis_index("ep"), lax.axis_index("tp")
    core = tp + 1 - 2 * lax.rem(tp, 2)
    across = lax.rem(tp + n_tp // 2, n_tp)
    corner = lax.rem(core + n_tp // 2, n_tp)
    return ep, tp, core, across, corner


def remote(src, dst, send, recv, ep, tp):
    return pltpu.make_async_remote_copy(
        src_ref=src, dst_ref=dst, send_sem=send, recv_sem=recv, device_id=(ep, tp), device_id_type=MESH
    )


def normed_rows(ref, columns, gain):
    values = ref[:, columns].astype(jnp.float32)
    inverse = lax.rsqrt(jnp.mean(values * values, axis=-1, keepdims=True) + EPSILON)
    return (values * inverse * gain).astype(jnp.bfloat16)


def layer_kernel(
    n_ep,
    n_tp,
    tokens_in,
    norm_gain,
    routes,
    route_weights,
    queries,
    keys_in,
    values_in,
    forget,
    query_gain,
    key_gain,
    gate_hbm,
    up_hbm,
    down_hbm,
    mixer_hbm,
    mixed,
    routed,
    gate_w,
    up_w,
    down_w,
    mixer,
    kv,
    kvbuf,
    q,
    fq,
    tok,
    meta,
    ysend,
    att,
    att_all,
    high,
    denom,
    accum,
    pieces,
    sums,
    near_own,
    near_far,
    sum_x,
    got_x,
    sum_r,
    back,
    x_send,
    x_recv,
    c_send,
    c_recv,
    d_send,
    d_recv,
    f_send,
    f_recv,
    n_send,
    n_recv,
    y_send,
    y_recv,
    r_send,
    r_recv,
    zu_send,
    zd_send,
    z_recv,
    mu_send,
    md_send,
    m_recv,
    b_send,
    b_recv,
    u_send,
    k_send,
    k_recv,
    t_send,
    t_recv,
    w_sem,
):
    ep, tp, core, across, corner = places(n_tp)
    rows, head_dim = keys_in.shape
    heads = forget.shape[0]
    part = rows // n_tp
    scale = head_dim ** (-0.5)
    local, width, ff = gate_w.shape
    per = local * CAP
    tokens = tokens_in.shape[0]
    choices = routes.shape[0]
    level, side = lax.div(ep, 2), lax.rem(ep, 2)
    levels = n_ep // 2
    beside = ep + 1 - 2 * side
    above = lax.rem(ep + 2, n_ep)
    below = lax.rem(ep + n_ep - 2, n_ep)
    both = jnp.minimum(level, levels - 1 - level)
    assert levels >= 4

    loads = [
        pltpu.make_async_copy(src, dst, w_sem.at[number])
        for number, (src, dst) in enumerate(
            [(gate_hbm, gate_w), (up_hbm, up_w), (down_hbm, down_w), (mixer_hbm, mixer)]
        )
    ]
    for load in loads:
        load.start()

    barrier = pltpu.get_barrier_semaphore()
    for step in range(1, n_ep):
        pl.semaphore_signal(
            barrier, inc=1, device_id=(lax.rem(ep + step, n_ep), tp), device_id_type=MESH
        )
    for step in range(1, n_tp):
        pl.semaphore_signal(
            barrier, inc=1, device_id=(ep, lax.rem(tp + step, n_tp)), device_id_type=MESH
        )

    def each(first, last, act):
        def body(number, carry):
            act(number)
            return carry

        lax.fori_loop(first, last, body, 0)

    def level_of(number):
        near = lax.div(number + 1, 2)
        odd = lax.rem(number, 2)
        far = number - both
        paired = level + near * (1 - 2 * odd)
        lone = jnp.where(level < levels - 1 - level, level + far, level - far)
        return jnp.where(number <= 2 * both, paired, lone)

    def z_up(source):
        return remote(tok.at[source], tok.at[source], zu_send.at[source], z_recv.at[source], above, tp)

    def z_down(source):
        return remote(tok.at[source], tok.at[source], zd_send.at[source], z_recv.at[source], below, tp)

    def m_up(source):
        return remote(meta.at[source], meta.at[source], mu_send.at[source], m_recv.at[source], above, tp)

    def m_down(source):
        return remote(meta.at[source], meta.at[source], md_send.at[source], m_recv.at[source], below, tp)

    def b_copy(number):
        slot = 2 * number + side
        return remote(
            ysend.at[number], pieces.at[tp, slot], b_send.at[number], b_recv.at[number], beside, tp
        )

    def up_copy(src, source):
        return remote(src, kvbuf.at[source], u_send.at[source], k_recv.at[source], above, tp)

    def side_copy(src, source):
        return remote(src, kvbuf.at[source], k_send.at[source], k_recv.at[source], beside, tp)

    def x_copy(slot):
        return remote(
            pieces.at[tp, slot], pieces.at[tp, slot], x_send.at[slot], x_recv.at[slot], ep, across
        )

    def c_copy(slot):
        return remote(
            pieces.at[tp, slot], pieces.at[tp, slot], c_send.at[slot], c_recv.at[slot], ep, core
        )

    def d_copy(slot):
        return remote(
            pieces.at[across, slot], pieces.at[across, slot], d_send.at[slot], d_recv.at[slot], ep, core
        )

    def far_copy(slot):
        return remote(sums.at[corner, slot], near_far.at[slot], f_send.at[slot], f_recv.at[slot], ep, core)

    def own_copy(slot):
        return remote(sums.at[core, slot], near_own.at[slot], n_send.at[slot], n_recv.at[slot], ep, core)

    def y_copy(slot):
        return remote(sum_x.at[slot], got_x.at[slot], y_send.at[slot], y_recv.at[slot], ep, across)

    def r_copy(slot, dest):
        return remote(sum_r.at[slot], back.at[ep], r_send.at[slot], r_recv.at[ep], dest, tp)

    def r_arrived(source):
        return remote(sum_r.at[0], back.at[source], r_send.at[0], r_recv.at[source], beside, tp)

    def t_copy(source, step):
        dest = lax.rem(tp + step, n_tp)
        return remote(att.at[dest], att_all.at[source], t_send.at[step], t_recv.at[source], ep, dest)

    strip = min(tokens, 32)
    for begin in range(0, tokens, strip):
        lines = slice(begin, begin + strip)
        values = tokens_in[lines, :].astype(jnp.float32)
        inverse = lax.rsqrt(jnp.mean(values * values, axis=-1, keepdims=True) + EPSILON)
        tok[level, lines, :] = (values * inverse * norm_gain[...]).astype(jnp.bfloat16)
    names = lax.broadcasted_iota(jnp.int32, (n_ep * local, tokens), 0)
    named = [names == routes[k : k + 1, :] for k in range(choices)]
    anyone = sum(jnp.where(mine, 1.0, 0.0) for mine in named).astype(jnp.bfloat16)
    earlier = jnp.where(
        lax.broadcasted_iota(jnp.int32, (tokens, tokens), 0)
        < lax.broadcasted_iota(jnp.int32, (tokens, tokens), 1),
        1.0,
        0.0,
    ).astype(jnp.bfloat16)
    prior = jnp.dot(anyone, earlier, preferred_element_type=jnp.float32)
    meta[level] = jnp.zeros(meta.shape[1:], jnp.float32)
    for k in range(choices):
        rank = jnp.sum(jnp.where(named[k], prior, 0.0), axis=0, keepdims=True)
        meta[level, k : k + 1, :] = routes[k : k + 1, :].astype(jnp.float32) * CAP + rank

    pl.semaphore_wait(barrier, n_ep + n_tp - 2)

    @pl.when(level + 1 < levels)
    def _():
        m_up(level).start()
        z_up(level).start()

    @pl.when(level > 0)
    def _():
        m_down(level).start()
        z_down(level).start()

    def select(source, place):
        lines = place * per + lax.broadcasted_iota(jnp.int32, (per, tokens), 0)
        lines = lines.astype(jnp.float32)
        picks = functools.reduce(
            jnp.logical_or, [lines == meta[source, k : k + 1, :] for k in range(choices)]
        )
        picks = jnp.where(picks, 1.0, 0.0).astype(jnp.bfloat16)
        return jnp.dot(picks, tok[source], preferred_element_type=jnp.float32).astype(jnp.bfloat16)

    def hand_out(source, number):
        slot = 2 * number + side
        pieces[tp, slot] = select(source, ep)
        x_copy(slot).start()
        c_copy(slot).start()
        ysend[number] = select(source, beside)
        b_copy(number).start()

    def from_side(number):
        slot = 2 * number + 1 - side
        b_copy(number).wait_recv()
        x_copy(slot).start()
        c_copy(slot).start()

    def relay(number):
        for other in (side, 1 - side):
            slot = 2 * number + other
            x_copy(slot).wait_recv()
            d_copy(slot).start()

    def expert(number, begin):
        own_rows = pl.ds(pl.multiple_of(number * CAP, CAP), CAP)
        taken = pieces[:, pl.ds(begin, 2), own_rows, :].reshape(n_tp * 2 * CAP, width)
        gate = jnp.dot(taken, gate_w[number], preferred_element_type=jnp.float32)
        upward = jnp.dot(taken, up_w[number], preferred_element_type=jnp.float32)
        hidden = (gate / (1.0 + jnp.exp(-gate)) * upward).astype(jnp.bfloat16)
        columns = min(width, 512)
        for begin_column in range(0, width, columns):
            lanes = slice(begin_column, begin_column + columns)
            result = lax.dot_general(
                hidden,
                down_w[number, lanes, :],
                (((1,), (1,)), ((), ())),
                preferred_element_type=jnp.float32,
            )
            sums[:, pl.ds(begin, 2), own_rows, lanes] = result.astype(jnp.bfloat16).reshape(
                n_tp, 2, CAP, columns
            )

    def experts(number):
        relay(number)
        for slot in (2 * number, 2 * number + 1):
            c_copy(slot).wait_recv()
            d_copy(slot).wait_recv()
        each(0, local, lambda which: expert(which, 2 * number))
        for slot in (2 * number, 2 * number + 1):
            far_copy(slot).start()
            own_copy(slot).start()

    def add(number):
        for other in (1 - side, side):
            slot = 2 * number + other
            far_copy(slot).wait_recv()
            sum_x[slot] = (
                sums[across, slot].astype(jnp.float32) + near_far[slot].astype(jnp.float32)
            ).astype(jnp.bfloat16)
            y_copy(slot).start()

    def total_of(slot):
        own_copy(slot).wait_recv()
        y_copy(slot).wait_recv()
        return (
            sums[tp, slot].astype(jnp.float32)
            + near_own[slot].astype(jnp.float32)
            + got_x[slot].astype(jnp.float32)
        ).astype(jnp.bfloat16)

    def send_back(number, other):
        slot = 2 * number + other
        sum_r[slot] = total_of(slot)
        r_copy(slot, 2 * level_of(number) + other).start()

    tile = rows // 2

    def block(source, keys_ref, diagonal):
        keys = keys_ref[:, :head_dim]
        vals = keys_ref[:, head_dim:]
        at = pl.ds(pl.multiple_of(source * rows, rows), rows)
        for head in range(heads):
            key_gate = forget[head : head + 1, at]
            for piece in range(2):
                span = pl.ds(head * rows + piece * tile, tile)
                scores = lax.dot_general(
                    q[span, :], keys, (((1,), (1,)), ((), ())), preferred_element_type=jnp.float32
                )
                scores = scores * scale + fq[span, 0:1] - key_gate
                if diagonal:
                    qpos = piece * tile + lax.broadcasted_iota(jnp.int32, scores.shape, 0)
                    kpos = lax.broadcasted_iota(jnp.int32, scores.shape, 1)
                    scores = jnp.where(kpos <= qpos, scores, NEGATIVE)
                top = jnp.max(scores, axis=1, keepdims=True)
                if diagonal:
                    newest = top
                else:
                    before = high[span, :]
                    newest = jnp.maximum(before, top)
                weights = jnp.exp(scores - newest)
                total = jnp.sum(weights, axis=1, keepdims=True)
                product = jnp.dot(
                    weights.astype(jnp.bfloat16), vals, preferred_element_type=jnp.float32
                )
                if not diagonal:
                    factor = jnp.exp(before - newest)
                    total = denom[span, :] * factor + total
                    product = accum[span, :] * factor + product
                high[span, :] = newest
                denom[span, :] = total
                accum[span, :] = product

    def keys_on(k):
        lower = ep - 2 * k
        side_copy(kv, lower).wait_recv()
        side_copy(kvbuf.at[lower], lower).start()

        @pl.when(level + 1 < levels)
        def _():
            up_copy(kvbuf.at[lower], lower).start()

    def attend(k):
        lower = ep - 2 * k
        block(lower, kvbuf.at[lower], False)
        other = 2 * (level - k) + 1 - side
        side_copy(kv, other).wait_recv()
        block(other, kvbuf.at[other], False)

    hand_out(level, 0)

    kv[:, :head_dim] = normed_rows(keys_in, slice(None), key_gain[...])
    kv[:, head_dim:] = values_in[...]

    @pl.when(side == 0)
    def _():
        side_copy(kv, ep).start()

    @pl.when(level == 0)
    def _():
        up_copy(kv, ep).start()

    mine = pl.ds(pl.multiple_of(ep * rows, rows), rows)
    for head in range(heads):
        lines = slice(head * rows, (head + 1) * rows)
        lanes = slice(head * head_dim, (head + 1) * head_dim)
        q[lines, :] = normed_rows(queries, lanes, query_gain[...])
        fq[lines, :] = jnp.broadcast_to(forget[head : head + 1, mine], (head_dim, rows)).T

    from_side(0)
    block(ep, kv, True)

    @pl.when(side == 1)
    def _():
        side_copy(kv, ep - 1).wait_recv()
        block(ep - 1, kvbuf.at[ep - 1], False)

    def reach(k):
        low, top = level - k, level + k
        low_at = jnp.where(k <= both, 2 * k - 1, both + k)
        top_at = jnp.where(k <= both, 2 * k, both + k)

        @pl.when(low >= 0)
        def _():
            m_up(low).wait_recv()
            z_up(low).wait_recv()

            @pl.when(level + 1 < levels)
            def _():
                m_up(low).start()
                z_up(low).start()

                @pl.when(low == 0)
                def _():
                    up_copy(kv, ep).start()

        @pl.when(top < levels)
        def _():
            m_down(top).wait_recv()
            z_down(top).wait_recv()

            @pl.when(level > 0)
            def _():
                m_down(top).start()
                z_down(top).start()

        @pl.when(low >= 0)
        def _():
            hand_out(low, low_at)

        @pl.when(top < levels)
        def _():
            hand_out(top, top_at)

        @pl.when(k == 1)
        def _():
            for load in loads:
                load.wait()

        @pl.when(k != 2)
        def _():
            experts(jnp.maximum(k - 2, 0))

        @pl.when(low >= 0)
        def _():
            from_side(low_at)

        @pl.when(top < levels)
        def _():
            from_side(top_at)

    each(1, levels, reach)

    @pl.when(level + 1 < levels)
    def _():
        each(1, level + 1, keys_on)

    def last(number):
        experts(number)
        add(number)

    each(levels - 2, levels, last)
    each(1, levels - 2, add)
    add(0)

    @pl.when(level + 1 == levels)
    def _():
        each(1, level + 1, keys_on)

    def turn(step):
        return jnp.where(step < 2, levels - 2 + step, step - 1)

    def send_both(step):
        number = turn(step)
        send_back(number, 1 - side)
        send_back(number, side)

    def early(step):
        send_both(step)
        for k in (2 * step + 1, 2 * step + 2):

            @pl.when(k <= level)
            def _():
                attend(k)

    each(0, levels // 2, early)
    for head in range(heads):
        span = pl.ds(head * rows, rows)
        result = (accum[span, :] / denom[span, :]).astype(jnp.bfloat16)
        for owner in range(n_tp):
            att[owner, head] = result[owner * part : (owner + 1) * part]
    for step in range(1, n_tp):
        t_copy(tp, step).start()
    att_all[tp] = att[tp]

    each(levels // 2, levels - 1, send_both)

    for step in range(1, n_tp):
        t_copy(lax.rem(tp - step + n_tp, n_tp), step).wait()
    total = None
    for source in range(n_tp):
        for head in range(heads):
            number = source * heads + head
            term = jnp.dot(
                att_all[source, head],
                mixer[number * head_dim : (number + 1) * head_dim, :],
                preferred_element_type=jnp.float32,
            )
            total = term if total is None else total + term
    mixed[...] = total.astype(jnp.bfloat16)

    send_back(0, 1 - side)
    back[ep] = total_of(side)

    def sent(slot):
        x_copy(slot).wait_send()
        c_copy(slot).wait_send()
        d_copy(slot).wait_send()
        far_copy(slot).wait_send()
        own_copy(slot).wait_send()
        y_copy(slot).wait_send()

        @pl.when(slot != side)
        def _():
            r_copy(slot, beside).wait_send()

    each(0, n_ep, sent)
    each(0, levels, lambda number: b_copy(number).wait_send())

    def passed(source):
        @pl.when(jnp.logical_and(source <= level, level + 1 < levels))
        def _():
            m_up(source).wait_send()
            z_up(source).wait_send()

        @pl.when(jnp.logical_and(source >= level, level > 0))
        def _():
            m_down(source).wait_send()
            z_down(source).wait_send()

    each(0, levels, passed)

    @pl.when(level + 1 < levels)
    def _():
        up_copy(kv, ep).wait_send()

    @pl.when(side == 0)
    def _():
        side_copy(kv, ep).wait_send()

    def keys_sent(k):
        source = ep - 2 * k
        side_copy(kv, source).wait_send()

        @pl.when(level + 1 < levels)
        def _():
            up_copy(kv, source).wait_send()

    each(1, level + 1, keys_sent)

    def arrived(source):
        @pl.when(source != ep)
        def _():
            r_arrived(source).wait_recv()

    each(0, n_ep, arrived)

    found_rows = back[...].reshape(n_ep * per, width)
    columns = jnp.concatenate(
        [meta[level, :choices, :], route_weights[...], jnp.zeros((8 - 2 * choices, tokens), jnp.float32)],
        axis=0,
    ).T
    lanes = lax.broadcasted_iota(jnp.int32, (tokens, n_ep * per), 1).astype(jnp.float32)
    summed = None
    for k in range(choices):
        pick = jnp.where(lanes == columns[:, k : k + 1], 1.0, 0.0).astype(jnp.bfloat16)
        found = jnp.dot(pick, found_rows, preferred_element_type=jnp.float32)
        term = found * columns[:, choices + k : choices + k + 1]
        summed = term if summed is None else summed + term
    routed[...] = summed.astype(jnp.bfloat16)


def on_device(
    n_ep,
    n_tp,
    queries,
    keys,
    values,
    forget_cache,
    query_gain,
    key_gain,
    mixer_out,
    expert_input,
    norm_gain,
    routes,
    route_weights,
    w_gate,
    w_up,
    w_down,
):
    rows, head_dim = keys.shape
    heads = forget_cache.shape[0]
    local, width, ff = w_gate.shape
    tokens = expert_input.shape[0]
    per = local * CAP
    part = rows // n_tp
    levels = n_ep // 2
    vmem = pl.BlockSpec(memory_space=pltpu.VMEM)
    anywhere = pl.BlockSpec(memory_space=pl.ANY)
    dma = pltpu.SemaphoreType.DMA
    buffer = pltpu.VMEM((n_ep, per, width), jnp.bfloat16)
    return pl.pallas_call(
        functools.partial(layer_kernel, n_ep, n_tp),
        out_shape=(
            jax.ShapeDtypeStruct((part, width), jnp.bfloat16),
            jax.ShapeDtypeStruct((tokens, width), jnp.bfloat16),
        ),
        in_specs=[vmem] * 10 + [anywhere] * 4,
        out_specs=(vmem, vmem),
        scratch_shapes=[pltpu.VMEM(w_gate.shape, jnp.bfloat16)] * 3
        + [
            pltpu.VMEM(mixer_out.shape, jnp.bfloat16),
            pltpu.VMEM((rows, 2 * head_dim), jnp.bfloat16),
            pltpu.VMEM((n_ep, rows, 2 * head_dim), jnp.bfloat16),
            pltpu.VMEM((heads * rows, head_dim), jnp.bfloat16),
            pltpu.VMEM((heads * rows, head_dim), jnp.float32),
            pltpu.VMEM((levels, tokens, width), jnp.bfloat16),
            pltpu.VMEM((levels, 8, tokens), jnp.float32),
            pltpu.VMEM((levels, per, width), jnp.bfloat16),
            pltpu.VMEM((n_tp, heads, part, head_dim), jnp.bfloat16),
            pltpu.VMEM((n_tp, heads, part, head_dim), jnp.bfloat16),
            pltpu.VMEM((heads * rows, 1), jnp.float32),
            pltpu.VMEM((heads * rows, 1), jnp.float32),
            pltpu.VMEM((heads * rows, head_dim), jnp.float32),
            pltpu.VMEM((n_tp, n_ep, per, width), jnp.bfloat16),
            pltpu.VMEM((n_tp, n_ep, per, width), jnp.bfloat16),
        ]
        + [buffer] * 6
        + [dma((n_ep,))] * 14
        + [dma((levels,))] * 8
        + [dma((n_ep,))] * 3
        + [dma((n_tp,))] * 2
        + [dma((4,))],
        compiler_params=pltpu.CompilerParams(
            collective_id=0, has_side_effects=True, vmem_limit_bytes=VMEM_LIMIT
        ),
        name="layer",
    )(
        expert_input,
        norm_gain.reshape(1, width),
        routes.T,
        route_weights.T,
        queries,
        keys,
        values,
        forget_cache,
        query_gain.reshape(1, head_dim),
        key_gain.reshape(1, head_dim),
        w_gate,
        w_up,
        w_down,
        mixer_out,
    )


def solution(mesh):
    n_ep, n_tp = mesh.shape["ep"], mesh.shape["tp"]
    in_specs = (
        P("ep", "tp"),
        P("ep", "tp"),
        P("ep", "tp"),
        P("tp", None),
        P(),
        P(),
        P(),
        P(("ep", "tp"), None),
        P(),
        P(("ep", "tp"), None),
        P(("ep", "tp"), None),
        P("ep", None, "tp"),
        P("ep", None, "tp"),
        P("ep", None, "tp"),
    )
    out_specs = (P(("ep", "tp"), None), P(("ep", "tp"), None))
    return jax.shard_map(
        functools.partial(on_device, n_ep, n_tp),
        mesh=mesh,
        in_specs=in_specs,
        out_specs=out_specs,
        check_vma=False,
    )
```

```python
import functools

import jax
import jax.numpy as jnp
from jax import lax
from jax.experimental import pallas as pl
from jax.experimental.pallas import tpu as pltpu
from jax.sharding import PartitionSpec as P

CAP = 16
EPSILON = 1e-06
NEGATIVE = -1e30
MESH = pl.DeviceIdType.MESH
VMEM_LIMIT = 62 * 1024 * 1024


def places(n_tp):
    ep, tp = lax.axis_index("ep"), lax.axis_index("tp")
    core = tp + 1 - 2 * lax.rem(tp, 2)
    across = lax.rem(tp + n_tp // 2, n_tp)
    corner = lax.rem(core + n_tp // 2, n_tp)
    return ep, tp, core, across, corner


def remote(src, dst, send, recv, ep, tp):
    return pltpu.make_async_remote_copy(
        src_ref=src, dst_ref=dst, send_sem=send, recv_sem=recv, device_id=(ep, tp), device_id_type=MESH
    )


def normed_rows(ref, columns, gain):
    values = ref[:, columns].astype(jnp.float32)
    inverse = lax.rsqrt(jnp.mean(values * values, axis=-1, keepdims=True) + EPSILON)
    return (values * inverse * gain).astype(jnp.bfloat16)


def layer_kernel(
    n_ep,
    n_tp,
    tokens_in,
    norm_gain,
    routes,
    route_weights,
    queries,
    keys_in,
    values_in,
    forget,
    query_gain,
    key_gain,
    gate_hbm,
    up_hbm,
    down_hbm,
    mixer_hbm,
    mixed,
    routed,
    gate_w,
    up_w,
    down_w,
    mixer,
    kv,
    kvbuf,
    q,
    fq,
    tok,
    meta,
    ysend,
    att,
    att_all,
    high,
    denom,
    accum,
    pieces,
    sums,
    near_own,
    near_far,
    sum_x,
    got_x,
    sum_r,
    back,
    x_send,
    x_recv,
    c_send,
    c_recv,
    d_send,
    d_recv,
    f_send,
    f_recv,
    n_send,
    n_recv,
    y_send,
    y_recv,
    r_send,
    r_recv,
    zu_send,
    zd_send,
    z_recv,
    mu_send,
    md_send,
    m_recv,
    b_send,
    b_recv,
    u_send,
    k_send,
    k_recv,
    t_send,
    t_recv,
    w_sem,
    mixed_v,
    routed_v,
    picked,
    o_sem,
):
    ep, tp, core, across, corner = places(n_tp)
    rows, head_dim = keys_in.shape
    heads = forget.shape[0]
    part = rows // n_tp
    scale = head_dim ** (-0.5)
    local, width, ff = gate_w.shape
    per = local * CAP
    tokens = tokens_in.shape[0]
    choices = routes.shape[0]
    level, side = lax.div(ep, 2), lax.rem(ep, 2)
    levels = n_ep // 2
    beside = ep + 1 - 2 * side
    above = lax.rem(ep + 2, n_ep)
    below = lax.rem(ep + n_ep - 2, n_ep)
    both = jnp.minimum(level, levels - 1 - level)
    assert levels >= 4
    halves = [slice(0, width // 2), slice(width // 2, width)]

    loads = [
        pltpu.make_async_copy(src, dst, w_sem.at[number])
        for number, (src, dst) in enumerate(
            [(gate_hbm, gate_w), (up_hbm, up_w), (down_hbm, down_w), (mixer_hbm, mixer)]
        )
    ]
    for load in loads:
        load.start()

    barrier = pltpu.get_barrier_semaphore()
    for step in range(1, n_ep):
        pl.semaphore_signal(
            barrier, inc=1, device_id=(lax.rem(ep + step, n_ep), tp), device_id_type=MESH
        )
    for step in range(1, n_tp):
        pl.semaphore_signal(
            barrier, inc=1, device_id=(ep, lax.rem(tp + step, n_tp)), device_id_type=MESH
        )

    def each(first, last, act):
        def body(number, carry):
            act(number)
            return carry

        lax.fori_loop(first, last, body, 0)

    def level_of(number):
        near = lax.div(number + 1, 2)
        odd = lax.rem(number, 2)
        far = number - both
        paired = level + near * (1 - 2 * odd)
        lone = jnp.where(level < levels - 1 - level, level + far, level - far)
        return jnp.where(number <= 2 * both, paired, lone)

    def z_up(source, half):
        lines = tok.at[source, :, halves[half]]
        number = 2 * source + half
        return remote(lines, lines, zu_send.at[number], z_recv.at[number], above, tp)

    def z_down(source, half):
        lines = tok.at[source, :, halves[half]]
        number = 2 * source + half
        return remote(lines, lines, zd_send.at[number], z_recv.at[number], below, tp)

    def m_up(source):
        return remote(meta.at[source], meta.at[source], mu_send.at[source], m_recv.at[source], above, tp)

    def m_down(source):
        return remote(meta.at[source], meta.at[source], md_send.at[source], m_recv.at[source], below, tp)

    def b_copy(number, half):
        slot = 2 * number + side
        piece = 2 * number + half
        return remote(
            ysend.at[number, :, halves[half]],
            pieces.at[tp, slot, :, halves[half]],
            b_send.at[piece],
            b_recv.at[piece],
            beside,
            tp,
        )

    def up_copy(src, source):
        return remote(src, kvbuf.at[source], u_send.at[source], k_recv.at[source], above, tp)

    def side_copy(src, source):
        return remote(src, kvbuf.at[source], k_send.at[source], k_recv.at[source], beside, tp)

    def x_copy(slot, lanes=slice(None)):
        piece = pieces.at[tp, slot, :, lanes]
        return remote(piece, piece, x_send.at[slot], x_recv.at[slot], ep, across)

    def c_copy(slot, lanes=slice(None)):
        piece = pieces.at[tp, slot, :, lanes]
        return remote(piece, piece, c_send.at[slot], c_recv.at[slot], ep, core)

    def d_copy(slot):
        return remote(
            pieces.at[across, slot], pieces.at[across, slot], d_send.at[slot], d_recv.at[slot], ep, core
        )

    def far_copy(slot):
        return remote(sums.at[corner, slot], near_far.at[slot], f_send.at[slot], f_recv.at[slot], ep, core)

    def own_copy(slot):
        return remote(sums.at[core, slot], near_own.at[slot], n_send.at[slot], n_recv.at[slot], ep, core)

    def y_copy(slot):
        return remote(sum_x.at[slot], got_x.at[slot], y_send.at[slot], y_recv.at[slot], ep, across)

    def r_copy(slot, dest):
        return remote(sum_r.at[slot], back.at[ep], r_send.at[slot], r_recv.at[ep], dest, tp)

    def r_arrived(source):
        return remote(sum_r.at[0], back.at[source], r_send.at[0], r_recv.at[source], beside, tp)

    def t_copy(source, step):
        dest = lax.rem(tp + step, n_tp)
        return remote(att.at[dest], att_all.at[source], t_send.at[step], t_recv.at[source], ep, dest)

    strip = min(tokens, 32)
    for begin in range(0, tokens, strip):
        lines = slice(begin, begin + strip)
        values = tokens_in[lines, :].astype(jnp.float32)
        inverse = lax.rsqrt(jnp.mean(values * values, axis=-1, keepdims=True) + EPSILON)
        tok[level, lines, :] = (values * inverse * norm_gain[...]).astype(jnp.bfloat16)
    names = lax.broadcasted_iota(jnp.int32, (n_ep * local, tokens), 0)
    named = [names == routes[k : k + 1, :] for k in range(choices)]
    anyone = sum(jnp.where(mine, 1.0, 0.0) for mine in named).astype(jnp.bfloat16)
    earlier = jnp.where(
        lax.broadcasted_iota(jnp.int32, (tokens, tokens), 0)
        < lax.broadcasted_iota(jnp.int32, (tokens, tokens), 1),
        1.0,
        0.0,
    ).astype(jnp.bfloat16)
    prior = jnp.dot(anyone, earlier, preferred_element_type=jnp.float32)
    meta[level] = jnp.zeros(meta.shape[1:], jnp.float32)
    for k in range(choices):
        rank = jnp.sum(jnp.where(named[k], prior, 0.0), axis=0, keepdims=True)
        meta[level, k : k + 1, :] = routes[k : k + 1, :].astype(jnp.float32) * CAP + rank

    pl.semaphore_wait(barrier, n_ep + n_tp - 2)

    @pl.when(level + 1 < levels)
    def _():
        m_up(level).start()
        for half in range(2):
            z_up(level, half).start()

    @pl.when(level > 0)
    def _():
        m_down(level).start()
        for half in range(2):
            z_down(level, half).start()

    def select(source, place, lanes):
        lines = place * per + lax.broadcasted_iota(jnp.int32, (per, tokens), 0)
        lines = lines.astype(jnp.float32)
        picks = functools.reduce(
            jnp.logical_or, [lines == meta[source, k : k + 1, :] for k in range(choices)]
        )
        picks = jnp.where(picks, 1.0, 0.0).astype(jnp.bfloat16)
        found = jnp.dot(picks, tok[source, :, lanes], preferred_element_type=jnp.float32)
        return found.astype(jnp.bfloat16)

    def hand_out(source, number, half):
        slot = 2 * number + side
        lanes = halves[half]
        ysend[number, :, lanes] = select(source, beside, lanes)
        b_copy(number, half).start()
        pieces[tp, slot, :, lanes] = select(source, ep, lanes)
        x_copy(slot, lanes).start()
        c_copy(slot, lanes).start()

    def from_side(number, half):
        slot = 2 * number + 1 - side
        b_copy(number, half).wait_recv()
        x_copy(slot, halves[half]).start()
        c_copy(slot, halves[half]).start()

    def relay(number):
        for other in (side, 1 - side):
            slot = 2 * number + other
            x_copy(slot).wait_recv()
            d_copy(slot).start()

    def expert(number, begin):
        own_rows = pl.ds(pl.multiple_of(number * CAP, CAP), CAP)
        taken = pieces[:, pl.ds(begin, 2), own_rows, :].reshape(n_tp * 2 * CAP, width)
        gate = jnp.dot(taken, gate_w[number], preferred_element_type=jnp.float32)
        upward = jnp.dot(taken, up_w[number], preferred_element_type=jnp.float32)
        hidden = (gate / (1.0 + jnp.exp(-gate)) * upward).astype(jnp.bfloat16)
        columns = min(width, 512)
        for begin_column in range(0, width, columns):
            lanes = slice(begin_column, begin_column + columns)
            result = lax.dot_general(
                hidden,
                down_w[number, lanes, :],
                (((1,), (1,)), ((), ())),
                preferred_element_type=jnp.float32,
            )
            sums[:, pl.ds(begin, 2), own_rows, lanes] = result.astype(jnp.bfloat16).reshape(
                n_tp, 2, CAP, columns
            )

    def experts(number):
        for slot in (2 * number, 2 * number + 1):
            c_copy(slot).wait_recv()
            d_copy(slot).wait_recv()
        each(0, local, lambda which: expert(which, 2 * number))
        for slot in (2 * number, 2 * number + 1):
            far_copy(slot).start()
            own_copy(slot).start()

    def add(number):
        for other in (1 - side, side):
            slot = 2 * number + other
            far_copy(slot).wait_recv()
            sum_x[slot] = (
                sums[across, slot].astype(jnp.float32) + near_far[slot].astype(jnp.float32)
            ).astype(jnp.bfloat16)
            y_copy(slot).start()

    def total_of(slot):
        own_copy(slot).wait_recv()
        y_copy(slot).wait_recv()
        return (
            sums[tp, slot].astype(jnp.float32)
            + near_own[slot].astype(jnp.float32)
            + got_x[slot].astype(jnp.float32)
        ).astype(jnp.bfloat16)

    def send_back(number, other):
        slot = 2 * number + other
        sum_r[slot] = total_of(slot)
        r_copy(slot, 2 * level_of(number) + other).start()

    tile = rows // 2

    def block(source, keys_ref, diagonal):
        keys = keys_ref[:, :head_dim]
        vals = keys_ref[:, head_dim:]
        at = pl.ds(pl.multiple_of(source * rows, rows), rows)
        for head in range(heads):
            key_gate = forget[head : head + 1, at]
            for piece in range(2):
                span = pl.ds(head * rows + piece * tile, tile)
                scores = lax.dot_general(
                    q[span, :], keys, (((1,), (1,)), ((), ())), preferred_element_type=jnp.float32
                )
                scores = scores * scale + fq[span, 0:1] - key_gate
                if diagonal:
                    qpos = piece * tile + lax.broadcasted_iota(jnp.int32, scores.shape, 0)
                    kpos = lax.broadcasted_iota(jnp.int32, scores.shape, 1)
                    scores = jnp.where(kpos <= qpos, scores, NEGATIVE)
                top = jnp.max(scores, axis=1, keepdims=True)
                if diagonal:
                    newest = top
                else:
                    before = high[span, :]
                    newest = jnp.maximum(before, top)
                weights = jnp.exp(scores - newest)
                total = jnp.sum(weights, axis=1, keepdims=True)
                product = jnp.dot(
                    weights.astype(jnp.bfloat16), vals, preferred_element_type=jnp.float32
                )
                if not diagonal:
                    factor = jnp.exp(before - newest)
                    total = denom[span, :] * factor + total
                    product = accum[span, :] * factor + product
                high[span, :] = newest
                denom[span, :] = total
                accum[span, :] = product

    def keys_on(k):
        lower = ep - 2 * k
        side_copy(kv, lower).wait_recv()
        side_copy(kvbuf.at[lower], lower).start()

        @pl.when(level + 1 < levels)
        def _():
            up_copy(kvbuf.at[lower], lower).start()

    def attend(k):
        lower = ep - 2 * k
        block(lower, kvbuf.at[lower], False)

    def attend_beside(k):
        other = 2 * (level - k) + 1 - side
        side_copy(kv, other).wait_recv()
        block(other, kvbuf.at[other], False)

    for half in range(2):
        hand_out(level, 0, half)

    kv[:, :head_dim] = normed_rows(keys_in, slice(None), key_gain[...])
    kv[:, head_dim:] = values_in[...]

    @pl.when(level == 0)
    def _():
        up_copy(kv, ep).start()

    mine = pl.ds(pl.multiple_of(ep * rows, rows), rows)
    for head in range(heads):
        lines = slice(head * rows, (head + 1) * rows)
        lanes = slice(head * head_dim, (head + 1) * head_dim)
        q[lines, :] = normed_rows(queries, lanes, query_gain[...])
        fq[lines, :] = jnp.broadcast_to(forget[head : head + 1, mine], (head_dim, rows)).T

    for half in range(2):
        from_side(0, half)
    block(ep, kv, True)

    def pass_on(k, half):
        low, top = level - k, level + k

        @pl.when(low >= 0)
        def _():
            if half == 0:
                m_up(low).wait_recv()
            z_up(low, half).wait_recv()

            @pl.when(level + 1 < levels)
            def _():
                if half == 0:
                    m_up(low).start()
                z_up(low, half).start()

        @pl.when(top < levels)
        def _():
            if half == 0:
                m_down(top).wait_recv()
            z_down(top, half).wait_recv()

            @pl.when(level > 0)
            def _():
                if half == 0:
                    m_down(top).start()
                z_down(top, half).start()

        if half == 1:

            @pl.when(jnp.logical_and(low == 0, level + 1 < levels))
            def _():
                up_copy(kv, ep).start()

    def reach(k):
        low, top = level - k, level + k
        first = jnp.where(k <= both, 2 * k - 1, both + k)
        for half in range(2):
            pass_on(k, half)

            @pl.when(low >= 0)
            def _():
                hand_out(low, first, half)

            @pl.when(top < levels)
            def _():
                hand_out(top, jnp.where(k <= both, 2 * k, both + k), half)

            if half == 0:

                @pl.when(k > 2)
                def _():
                    experts(k - 2)

            if half == 1:
                relay(k - 1)

                @pl.when(k == 1)
                def _():
                    for load in loads:
                        load.wait()

                @pl.when(jnp.logical_or(k == 1, k == levels - 1))
                def _():
                    experts(k - 1)

                interior = jnp.logical_and(k > level, k <= 2 * level)

                @pl.when(jnp.logical_and(level + 1 < levels, interior))
                def _():
                    keys_on(k - level)

            @pl.when(jnp.logical_or(low >= 0, top < levels))
            def _():
                from_side(first, half)

            @pl.when(k <= both)
            def _():
                from_side(2 * k, half)

    each(1, levels, reach)

    @pl.when(side == 0)
    def _():
        side_copy(kv, ep).start()

    @pl.when(level + 1 < levels)
    def _():
        each(jnp.maximum(levels - level, 1), level + 1, keys_on)

    def send_both(number):
        send_back(number, 1 - side)
        send_back(number, side)

    def top_keys(begin, end):
        @pl.when(level + 1 == levels)
        def _():
            each(begin, end, keys_on)

    add(levels - 2)
    top_keys(1, levels // 2)
    relay(levels - 1)
    experts(levels - 1)
    send_back(levels - 2, 1 - side)
    add(levels - 1)
    each(1, levels - 2, add)
    send_back(levels - 2, side)
    top_keys(levels // 2, levels)
    each(1, level + 1, attend)
    send_back(levels - 1, 1 - side)
    each(1 - side, lax.div(level, 2) + 1, attend_beside)
    send_back(levels - 1, side)
    each(lax.div(level, 2) + 1, level + 1, attend_beside)
    for head in range(heads):
        span = pl.ds(head * rows, rows)
        result = (accum[span, :] / denom[span, :]).astype(jnp.bfloat16)
        for owner in range(n_tp):
            att[owner, head] = result[owner * part : (owner + 1) * part]
    for step in range(1, n_tp):
        t_copy(tp, step).start()
    att_all[tp] = att[tp]
    add(0)
    each(1, levels - 2, send_both)

    for step in range(1, n_tp):
        t_copy(lax.rem(tp - step + n_tp, n_tp), step).wait()
    chunk = min(width, 512)
    strips = [slice(begin, begin + chunk) for begin in range(0, width, chunk)]
    for lanes in strips:
        total = None
        for source in range(n_tp):
            for head in range(heads):
                number = source * heads + head
                term = jnp.dot(
                    att_all[source, head],
                    mixer[number * head_dim : (number + 1) * head_dim, lanes],
                    preferred_element_type=jnp.float32,
                )
                total = term if total is None else total + term
        mixed_v[:, lanes] = total.astype(jnp.bfloat16)
    mixed_out = pltpu.make_async_copy(mixed_v, mixed, o_sem.at[len(strips)])
    mixed_out.start()

    columns = jnp.concatenate(
        [meta[level, :choices, :], route_weights[...], jnp.zeros((8 - 2 * choices, tokens), jnp.float32)],
        axis=0,
    ).T
    slots = lax.broadcasted_iota(jnp.int32, (tokens, n_ep * per), 1).astype(jnp.float32)
    for k in range(choices):
        picked[k] = jnp.where(slots == columns[:, k : k + 1], 1.0, 0.0).astype(jnp.bfloat16)

    send_back(0, 1 - side)
    back[ep] = total_of(side)

    def arrived(source):
        @pl.when(source != ep)
        def _():
            r_arrived(source).wait_recv()

    each(0, n_ep, arrived)

    outs = []
    for strip_number, lanes in enumerate(strips):
        found_rows = back[:, :, lanes].reshape(n_ep * per, chunk)
        summed = None
        for k in range(choices):
            found = jnp.dot(picked[k], found_rows, preferred_element_type=jnp.float32)
            term = found * columns[:, choices + k : choices + k + 1]
            summed = term if summed is None else summed + term
        routed_v[:, lanes] = summed.astype(jnp.bfloat16)
        out = pltpu.make_async_copy(routed_v.at[:, lanes], routed.at[:, lanes], o_sem.at[strip_number])
        out.start()
        outs.append(out)

    def sent(slot):
        x_copy(slot).wait_send()
        c_copy(slot).wait_send()
        d_copy(slot).wait_send()
        far_copy(slot).wait_send()
        own_copy(slot).wait_send()
        y_copy(slot).wait_send()

        @pl.when(slot != side)
        def _():
            r_copy(slot, beside).wait_send()

    each(0, n_ep, sent)
    for half in range(2):
        each(0, levels, lambda number: b_copy(number, half).wait_send())

    def passed(source):
        @pl.when(jnp.logical_and(source <= level, level + 1 < levels))
        def _():
            m_up(source).wait_send()
            for half in range(2):
                z_up(source, half).wait_send()

        @pl.when(jnp.logical_and(source >= level, level > 0))
        def _():
            m_down(source).wait_send()
            for half in range(2):
                z_down(source, half).wait_send()

    each(0, levels, passed)

    @pl.when(level + 1 < levels)
    def _():
        up_copy(kv, ep).wait_send()

    @pl.when(side == 0)
    def _():
        side_copy(kv, ep).wait_send()

    def keys_sent(k):
        source = ep - 2 * k
        side_copy(kv, source).wait_send()

        @pl.when(level + 1 < levels)
        def _():
            up_copy(kv, source).wait_send()

    each(1, level + 1, keys_sent)

    mixed_out.wait()
    for out in outs:
        out.wait()


def hand_off(mixed, routed, mixed_out, routed_out, mixed_v, routed_v, in_sem, out_sem):
    parts = 2
    moves = []
    for which, (src, held, dst) in enumerate(
        [(mixed, mixed_v, mixed_out), (routed, routed_v, routed_out)]
    ):
        lines = src.shape[0] // parts
        for number in range(parts):
            span = slice(number * lines, (number + 1) * lines)
            at = which * parts + number
            moves.append(
                (
                    pltpu.make_async_copy(src.at[span], held.at[span], in_sem.at[at]),
                    pltpu.make_async_copy(held.at[span], dst.at[span], out_sem.at[at]),
                )
            )
    for load, _ in moves:
        load.start()
    for load, store in moves:
        load.wait()
        store.start()
    for _, store in moves:
        store.wait()


def on_device(
    n_ep,
    n_tp,
    queries,
    keys,
    values,
    forget_cache,
    query_gain,
    key_gain,
    mixer_out,
    expert_input,
    norm_gain,
    routes,
    route_weights,
    w_gate,
    w_up,
    w_down,
):
    rows, head_dim = keys.shape
    heads = forget_cache.shape[0]
    local, width, ff = w_gate.shape
    tokens = expert_input.shape[0]
    per = local * CAP
    part = rows // n_tp
    levels = n_ep // 2
    vmem = pl.BlockSpec(memory_space=pltpu.VMEM)
    anywhere = pl.BlockSpec(memory_space=pl.ANY)
    dma = pltpu.SemaphoreType.DMA
    buffer = pltpu.VMEM((n_ep, per, width), jnp.bfloat16)
    mixed, routed = pl.pallas_call(
        functools.partial(layer_kernel, n_ep, n_tp),
        out_shape=(
            jax.ShapeDtypeStruct((part, width), jnp.bfloat16),
            jax.ShapeDtypeStruct((tokens, width), jnp.bfloat16),
        ),
        in_specs=[vmem] * 10 + [anywhere] * 4,
        out_specs=(anywhere, anywhere),
        scratch_shapes=[pltpu.VMEM(w_gate.shape, jnp.bfloat16)] * 3
        + [
            pltpu.VMEM(mixer_out.shape, jnp.bfloat16),
            pltpu.VMEM((rows, 2 * head_dim), jnp.bfloat16),
            pltpu.VMEM((n_ep, rows, 2 * head_dim), jnp.bfloat16),
            pltpu.VMEM((heads * rows, head_dim), jnp.bfloat16),
            pltpu.VMEM((heads * rows, head_dim), jnp.float32),
            pltpu.VMEM((levels, tokens, width), jnp.bfloat16),
            pltpu.VMEM((levels, 8, tokens), jnp.float32),
            pltpu.VMEM((levels, per, width), jnp.bfloat16),
            pltpu.VMEM((n_tp, heads, part, head_dim), jnp.bfloat16),
            pltpu.VMEM((n_tp, heads, part, head_dim), jnp.bfloat16),
            pltpu.VMEM((heads * rows, 1), jnp.float32),
            pltpu.VMEM((heads * rows, 1), jnp.float32),
            pltpu.VMEM((heads * rows, head_dim), jnp.float32),
            pltpu.VMEM((n_tp, n_ep, per, width), jnp.bfloat16),
            pltpu.VMEM((n_tp, n_ep, per, width), jnp.bfloat16),
        ]
        + [buffer] * 6
        + [dma((n_ep,))] * 17
        + [dma((levels,))] * 3
        + [dma((n_ep,))] * 5
        + [dma((n_tp,))] * 2
        + [
            dma((4,)),
            pltpu.VMEM((part, width), jnp.bfloat16),
            pltpu.VMEM((tokens, width), jnp.bfloat16),
            pltpu.VMEM((routes.shape[1], tokens, n_ep * per), jnp.bfloat16),
            dma((width // min(width, 512) + 1,)),
        ],
        compiler_params=pltpu.CompilerParams(
            collective_id=0, has_side_effects=True, vmem_limit_bytes=VMEM_LIMIT
        ),
        name="layer",
    )(
        expert_input,
        norm_gain.reshape(1, width),
        routes.T,
        route_weights.T,
        queries,
        keys,
        values,
        forget_cache,
        query_gain.reshape(1, head_dim),
        key_gain.reshape(1, head_dim),
        w_gate,
        w_up,
        w_down,
        mixer_out,
    )
    return pl.pallas_call(
        hand_off,
        out_shape=tuple(jax.ShapeDtypeStruct(part.shape, part.dtype) for part in (mixed, routed)),
        in_specs=[anywhere] * 2,
        out_specs=(anywhere, anywhere),
        scratch_shapes=[pltpu.VMEM(part.shape, part.dtype) for part in (mixed, routed)]
        + [dma((4,))] * 2,
        name="hand_off",
    )(mixed, routed)


def solution(mesh):
    n_ep, n_tp = mesh.shape["ep"], mesh.shape["tp"]
    in_specs = (
        P("ep", "tp"),
        P("ep", "tp"),
        P("ep", "tp"),
        P("tp", None),
        P(),
        P(),
        P(),
        P(("ep", "tp"), None),
        P(),
        P(("ep", "tp"), None),
        P(("ep", "tp"), None),
        P("ep", None, "tp"),
        P("ep", None, "tp"),
        P("ep", None, "tp"),
    )
    out_specs = (P(("ep", "tp"), None), P(("ep", "tp"), None))
    return jax.shard_map(
        functools.partial(on_device, n_ep, n_tp),
        mesh=mesh,
        in_specs=in_specs,
        out_specs=out_specs,
        check_vma=False,
    )
```

```python
import functools

import jax
import jax.numpy as jnp
from jax import lax
from jax.experimental import pallas as pl
from jax.experimental.pallas import tpu as pltpu
from jax.sharding import PartitionSpec as P

CAP = 16
EPSILON = 1e-06
NEGATIVE = -1e30
MESH = pl.DeviceIdType.MESH
VMEM_LIMIT = 63 * 1024 * 1024


def places(n_tp):
    ep, tp = lax.axis_index("ep"), lax.axis_index("tp")
    core = tp + 1 - 2 * lax.rem(tp, 2)
    across = lax.rem(tp + n_tp // 2, n_tp)
    corner = lax.rem(core + n_tp // 2, n_tp)
    return ep, tp, core, across, corner


def remote(src, dst, send, recv, ep, tp):
    return pltpu.make_async_remote_copy(
        src_ref=src, dst_ref=dst, send_sem=send, recv_sem=recv, device_id=(ep, tp), device_id_type=MESH
    )


def normed_rows(ref, columns, gain):
    values = ref[:, columns].astype(jnp.float32)
    inverse = lax.rsqrt(jnp.mean(values * values, axis=-1, keepdims=True) + EPSILON)
    return (values * inverse * gain).astype(jnp.bfloat16)


def layer_kernel(
    n_ep,
    n_tp,
    tokens_in,
    norm_gain,
    routes,
    route_weights,
    queries,
    keys_in,
    values_in,
    forget,
    query_gain,
    key_gain,
    gate_hbm,
    up_hbm,
    down_hbm,
    mixer_hbm,
    mixed,
    routed,
    gate_w,
    up_w,
    down_w,
    mixer,
    kv,
    kvbuf,
    q,
    fq,
    tok,
    meta,
    ysend,
    att,
    att_all,
    high,
    denom,
    accum,
    pieces,
    sums,
    near_own,
    near_far,
    sum_x,
    got_x,
    sum_r,
    back,
    x_send,
    x_recv,
    c_send,
    c_recv,
    d_send,
    d_recv,
    f_send,
    f_recv,
    n_send,
    n_recv,
    y_send,
    y_recv,
    r_send,
    r_recv,
    zu_send,
    zd_send,
    z_recv,
    mu_send,
    md_send,
    m_recv,
    b_send,
    b_recv,
    u_send,
    k_send,
    k_recv,
    t_send,
    t_recv,
    w_sem,
    mixed_v,
    routed_v,
    picked,
    weighing,
    gathered,
    o_sem,
    pair_rows,
    part_v,
    far_in,
    merged,
    p_send,
    p_recv,
    g_send,
    g_recv,
    h_recv,
):
    ep, tp, core, across, corner = places(n_tp)
    rows, head_dim = keys_in.shape
    heads = forget.shape[0]
    part = rows // n_tp
    scale = head_dim ** (-0.5)
    local, width, ff = gate_w.shape
    per = local * CAP
    tokens = tokens_in.shape[0]
    choices = routes.shape[0]
    level, side = lax.div(ep, 2), lax.rem(ep, 2)
    levels = n_ep // 2
    beside = ep + 1 - 2 * side
    above = lax.rem(ep + 2, n_ep)
    below = lax.rem(ep + n_ep - 2, n_ep)
    both = jnp.minimum(level, levels - 1 - level)
    edge, joins = both == 0, both <= 1
    assert levels >= 4
    halves = [slice(0, width // 2), slice(width // 2, width)]

    loads = [
        pltpu.make_async_copy(src, dst, w_sem.at[number])
        for number, (src, dst) in enumerate(
            [(gate_hbm, gate_w), (up_hbm, up_w), (down_hbm, down_w), (mixer_hbm, mixer)]
        )
    ]
    for load in loads:
        load.start()

    barrier = pltpu.get_barrier_semaphore()
    for step in range(1, n_ep):
        pl.semaphore_signal(
            barrier, inc=1, device_id=(lax.rem(ep + step, n_ep), tp), device_id_type=MESH
        )
    for step in range(1, n_tp):
        pl.semaphore_signal(
            barrier, inc=1, device_id=(ep, lax.rem(tp + step, n_tp)), device_id_type=MESH
        )

    def each(first, last, act):
        def body(number, carry):
            act(number)
            return carry

        lax.fori_loop(first, last, body, 0)

    def level_of(number):
        near = lax.div(number + 1, 2)
        odd = lax.rem(number, 2)
        far = number - both
        paired = level + near * (1 - 2 * odd)
        lone = jnp.where(level < levels - 1 - level, level + far, level - far)
        return jnp.where(number <= 2 * both, paired, lone)

    def z_up(source, half):
        lines = tok.at[source, :, halves[half]]
        return remote(lines, lines, zu_send.at[source], z_recv.at[2 * source + half], above, tp)

    def z_down(source, half):
        lines = tok.at[source, :, halves[half]]
        return remote(lines, lines, zd_send.at[source], z_recv.at[2 * source + half], below, tp)

    def passed_all(source, sems):
        block = tok.at[source]
        return remote(block, block, sems.at[source], z_recv.at[0], above, tp)

    def m_up(source):
        return remote(meta.at[source], meta.at[source], mu_send.at[source], m_recv.at[source], above, tp)

    def m_down(source):
        return remote(meta.at[source], meta.at[source], md_send.at[source], m_recv.at[source], below, tp)

    def b_copy(number, half):
        slot = 2 * number + side
        piece = 2 * number + half
        return remote(
            ysend.at[number, :, halves[half]],
            pieces.at[tp, slot, :, halves[half]],
            b_send.at[0],
            b_recv.at[piece],
            beside,
            tp,
        )

    def up_copy(src, source):
        return remote(src, kvbuf.at[source], u_send.at[lax.div(source, 2)], k_recv.at[source], above, tp)

    def side_copy(src, source):
        return remote(src, kvbuf.at[source], k_send.at[lax.div(source, 2)], k_recv.at[source], beside, tp)

    def x_move(src, dst, slot):
        return remote(src, dst, x_send.at[0], x_recv.at[lax.div(slot, 2)], ep, across)

    def c_move(src, dst, slot):
        return remote(src, dst, c_send.at[0], c_recv.at[lax.div(slot, 2)], ep, core)

    def d_move(src, dst, slot):
        return remote(src, dst, d_send.at[0], d_recv.at[lax.div(slot, 2)], ep, core)

    def f_move(src, dst, slot):
        return remote(src, dst, f_send.at[0], f_recv.at[lax.div(slot, 2)], ep, core)

    def n_move(src, dst, slot):
        return remote(src, dst, n_send.at[0], n_recv.at[lax.div(slot, 2)], ep, core)

    def x_copy(slot, lanes):
        piece = pieces.at[tp, slot, :, lanes]
        return x_move(piece, piece, slot)

    def c_copy(slot, lanes):
        piece = pieces.at[tp, slot, :, lanes]
        return c_move(piece, piece, slot)

    def d_copy(slot):
        piece = pieces.at[across, slot]
        return d_move(piece, piece, slot)

    def far_copy(slot):
        return f_move(sums.at[corner, slot], near_far.at[slot], slot)

    def own_copy(slot):
        return n_move(sums.at[core, slot], near_own.at[slot], slot)

    def pair(buffer, number):
        return buffer.at[pl.ds(2 * number, 2)]

    def y_copy(slot, half):
        lanes, piece = halves[half], 2 * slot + half
        return remote(
            sum_x.at[slot, :, lanes],
            got_x.at[slot, :, lanes],
            y_send.at[0],
            y_recv.at[piece],
            ep,
            across,
        )

    def r_copy(slot, dest, lanes=slice(None)):
        src, dst = sum_r.at[slot, :, lanes], back.at[ep, :, lanes]
        return remote(src, dst, r_send.at[0], r_recv.at[level], dest, tp)

    def r_arrived(rows_of, source):
        return remote(rows_of, rows_of, r_send.at[0], r_recv.at[source], beside, tp)

    def t_copy(source, step):
        dest = lax.rem(tp + step, n_tp)
        return remote(att.at[dest], att_all.at[source], t_send.at[step], t_recv.at[source], ep, dest)

    strip = min(tokens, 32)
    for begin in range(0, tokens, strip):
        lines = slice(begin, begin + strip)
        values = tokens_in[lines, :].astype(jnp.float32)
        inverse = lax.rsqrt(jnp.mean(values * values, axis=-1, keepdims=True) + EPSILON)
        tok[level, lines, :] = (values * inverse * norm_gain[...]).astype(jnp.bfloat16)
    names = lax.broadcasted_iota(jnp.int32, (n_ep * local, tokens), 0)
    named = [names == routes[k : k + 1, :] for k in range(choices)]
    anyone = sum(jnp.where(mine, 1.0, 0.0) for mine in named).astype(jnp.bfloat16)
    earlier = jnp.where(
        lax.broadcasted_iota(jnp.int32, (tokens, tokens), 0)
        < lax.broadcasted_iota(jnp.int32, (tokens, tokens), 1),
        1.0,
        0.0,
    ).astype(jnp.bfloat16)
    prior = jnp.dot(anyone, earlier, preferred_element_type=jnp.float32)
    meta[level] = jnp.zeros(meta.shape[1:], jnp.float32)
    for k in range(choices):
        rank = jnp.sum(jnp.where(named[k], prior, 0.0), axis=0, keepdims=True)
        meta[level, k : k + 1, :] = routes[k : k + 1, :].astype(jnp.float32) * CAP + rank
    meta[level, choices : 2 * choices, :] = route_weights[...]

    pl.semaphore_wait(barrier, n_ep + n_tp - 2)

    @pl.when(level + 1 < levels)
    def _():
        m_up(level).start()
        for half in range(2):
            z_up(level, half).start()

    @pl.when(level > 0)
    def _():
        m_down(level).start()
        for half in range(2):
            z_down(level, half).start()

    def select(source, place, lanes):
        lines = place * per + lax.broadcasted_iota(jnp.int32, (per, tokens), 0)
        lines = lines.astype(jnp.float32)
        picks = functools.reduce(
            jnp.logical_or, [lines == meta[source, k : k + 1, :] for k in range(choices)]
        )
        picks = jnp.where(picks, 1.0, 0.0).astype(jnp.bfloat16)
        found = jnp.dot(picks, tok[source, :, lanes], preferred_element_type=jnp.float32)
        return found.astype(jnp.bfloat16)

    def hand_out(source, number, half):
        slot = 2 * number + side
        lanes = halves[half]
        ysend[number, :, lanes] = select(source, beside, lanes)
        b_copy(number, half).start()
        pieces[tp, slot, :, lanes] = select(source, ep, lanes)
        x_copy(slot, lanes).start()
        c_copy(slot, lanes).start()

    def from_side(number, half):
        slot = 2 * number + 1 - side
        b_copy(number, half).wait_recv()
        x_copy(slot, halves[half]).start()
        c_copy(slot, halves[half]).start()

    def relay(number):
        whole = pair(pieces.at[across], number)
        x_move(whole, whole, 2 * number).wait_recv()
        for slot in (2 * number, 2 * number + 1):
            d_copy(slot).start()

    def expert(number, begin):
        own_rows = pl.ds(pl.multiple_of(number * CAP, CAP), CAP)
        taken = pieces[:, pl.ds(begin, 2), own_rows, :].reshape(n_tp * 2 * CAP, width)
        gate = jnp.dot(taken, gate_w[number], preferred_element_type=jnp.float32)
        upward = jnp.dot(taken, up_w[number], preferred_element_type=jnp.float32)
        hidden = (gate / (1.0 + jnp.exp(-gate)) * upward).astype(jnp.bfloat16)
        columns = min(width, 512)
        for begin_column in range(0, width, columns):
            lanes = slice(begin_column, begin_column + columns)
            result = lax.dot_general(
                hidden,
                down_w[number, lanes, :],
                (((1,), (1,)), ((), ())),
                preferred_element_type=jnp.float32,
            )
            sums[:, pl.ds(begin, 2), own_rows, lanes] = result.astype(jnp.bfloat16).reshape(
                n_tp, 2, CAP, columns
            )

    def experts(number):
        whole = pair(pieces.at[core], number)
        c_move(whole, whole, 2 * number).wait_recv()
        d_move(whole, whole, 2 * number).wait_recv()
        each(0, local, lambda which: expert(which, 2 * number))
        for slot in (2 * number, 2 * number + 1):
            far_copy(slot).start()
            own_copy(slot).start()

    def add(number):
        whole = pair(near_far, number)
        f_move(whole, whole, 2 * number).wait_recv()
        for other in (1 - side, side):
            slot = 2 * number + other
            for half in range(2):
                lanes = halves[half]
                sum_x[slot, :, lanes] = (
                    sums[across, slot, :, lanes].astype(jnp.float32)
                    + near_far[slot, :, lanes].astype(jnp.float32)
                ).astype(jnp.bfloat16)
                y_copy(slot, half).start()

    def own_landed(number, other):
        @pl.when(other != side)
        def _():
            whole = pair(near_own, number)
            n_move(whole, whole, 2 * number).wait_recv()

    def total_of(slot, half):
        lanes = halves[half]
        y_copy(slot, half).wait_recv()
        return (
            sums[tp, slot, :, lanes].astype(jnp.float32)
            + near_own[slot, :, lanes].astype(jnp.float32)
            + got_x[slot, :, lanes].astype(jnp.float32)
        ).astype(jnp.bfloat16)

    def send_back(number, other):
        slot = 2 * number + other
        own_landed(number, other)
        for half in range(2):
            sum_r[slot, :, halves[half]] = total_of(slot, half)
            r_copy(slot, 2 * level_of(number) + other, halves[half]).start()

    goal = level_of(levels - 1)
    toward = jnp.where(level == 0, above, below)

    def p_copy(half):
        src = sum_r.at[2 * levels - 1 - side, :, halves[half]]
        dst = pair_rows.at[side, :, halves[half]]
        return remote(src, dst, p_send.at[0], p_recv.at[half], beside, tp)

    def g_copy(half):
        src, dst = part_v.at[:, halves[half]], far_in.at[:, halves[half]]
        return remote(src, dst, g_send.at[0], g_recv.at[half], toward, tp)

    def h_copy(half):
        src, dst = part_v.at[:, halves[half]], merged.at[:, halves[half]]
        return remote(src, dst, g_send.at[0], h_recv.at[0], 2 * goal + side, tp)

    def weighed(half):
        p_copy(half).wait_recv()
        columns = meta[goal].T
        names = 2 * per * level + lax.broadcasted_iota(jnp.int32, (tokens, 2 * per), 1)
        names = names.astype(jnp.float32)
        rows_of = pair_rows[:, :, halves[half]].reshape(2 * per, width // 2)
        summed = None
        for k in range(choices):
            pick = jnp.where(names == columns[:, k : k + 1], 1.0, 0.0).astype(jnp.bfloat16)
            found = jnp.dot(pick, rows_of, preferred_element_type=jnp.float32)
            term = found * columns[:, choices + k : choices + k + 1]
            summed = term if summed is None else summed + term
        return summed

    def merge_out(half):
        part_v[:, halves[half]] = weighed(half).astype(jnp.bfloat16)
        g_copy(half).start()

    def merge_on(half):
        @pl.when(jnp.logical_and(joins, jnp.logical_not(edge)))
        def _():
            summed = weighed(half)
            g_copy(half).wait_recv()
            summed = summed + far_in[:, halves[half]].astype(jnp.float32)
            part_v[:, halves[half]] = summed.astype(jnp.bfloat16)
            h_copy(half).start()

    def far_first():
        @pl.when(joins)
        def _():
            slot = 2 * levels - 1 - side
            own_landed(levels - 1, 1 - side)
            for half in range(2):
                sum_r[slot, :, halves[half]] = total_of(slot, half)
                p_copy(half).start()

        @pl.when(jnp.logical_not(joins))
        def _():
            send_back(levels - 1, 1 - side)

    def far_second():
        @pl.when(joins)
        def _():
            for half in range(2):
                pair_rows[side, :, halves[half]] = total_of(2 * levels - 2 + side, half)

        @pl.when(jnp.logical_not(joins))
        def _():
            send_back(levels - 1, side)

        @pl.when(edge)
        def _():
            for half in range(2):
                merge_out(half)

    tile = rows // 2

    def block(source, keys_ref, diagonal):
        keys = keys_ref[:, :head_dim]
        vals = keys_ref[:, head_dim:]
        at = pl.ds(pl.multiple_of(source * rows, rows), rows)
        for head in range(heads):
            key_gate = forget[head : head + 1, at]
            for piece in range(2):
                span = pl.ds(head * rows + piece * tile, tile)
                scores = lax.dot_general(
                    q[span, :], keys, (((1,), (1,)), ((), ())), preferred_element_type=jnp.float32
                )
                scores = scores * scale + fq[span, 0:1] - key_gate
                if diagonal:
                    qpos = piece * tile + lax.broadcasted_iota(jnp.int32, scores.shape, 0)
                    kpos = lax.broadcasted_iota(jnp.int32, scores.shape, 1)
                    scores = jnp.where(kpos <= qpos, scores, NEGATIVE)
                top = jnp.max(scores, axis=1, keepdims=True)
                if diagonal:
                    newest = top
                else:
                    before = high[span, :]
                    newest = jnp.maximum(before, top)
                weights = jnp.exp(scores - newest)
                total = jnp.sum(weights, axis=1, keepdims=True)
                product = jnp.dot(
                    weights.astype(jnp.bfloat16), vals, preferred_element_type=jnp.float32
                )
                if not diagonal:
                    factor = jnp.exp(before - newest)
                    total = denom[span, :] * factor + total
                    product = accum[span, :] * factor + product
                high[span, :] = newest
                denom[span, :] = total
                accum[span, :] = product

    def keys_on(k):
        lower = ep - 2 * k
        side_copy(kv, lower).wait_recv()
        side_copy(kvbuf.at[lower], lower).start()

        @pl.when(level + 1 < levels)
        def _():
            up_copy(kvbuf.at[lower], lower).start()

    def attend(k):
        lower = ep - 2 * k
        block(lower, kvbuf.at[lower], False)

    def attend_beside(k):
        other = 2 * (level - k) + 1 - side
        side_copy(kv, other).wait_recv()
        block(other, kvbuf.at[other], False)

    for half in range(2):
        hand_out(level, 0, half)

    kv[:, :head_dim] = normed_rows(keys_in, slice(None), key_gain[...])
    kv[:, head_dim:] = values_in[...]

    @pl.when(level == 0)
    def _():
        up_copy(kv, ep).start()

    mine = pl.ds(pl.multiple_of(ep * rows, rows), rows)
    for head in range(heads):
        lines = slice(head * rows, (head + 1) * rows)
        lanes = slice(head * head_dim, (head + 1) * head_dim)
        q[lines, :] = normed_rows(queries, lanes, query_gain[...])
        fq[lines, :] = jnp.broadcast_to(forget[head : head + 1, mine], (head_dim, rows)).T

    for half in range(2):
        from_side(0, half)
    block(ep, kv, True)

    def pass_on(k, half):
        low, top = level - k, level + k

        @pl.when(low >= 0)
        def _():
            if half == 0:
                m_up(low).wait_recv()
            z_up(low, half).wait_recv()

            @pl.when(level + 1 < levels)
            def _():
                if half == 0:
                    m_up(low).start()
                z_up(low, half).start()

        @pl.when(top < levels)
        def _():
            if half == 0:
                m_down(top).wait_recv()
            z_down(top, half).wait_recv()

            @pl.when(level > 0)
            def _():
                if half == 0:
                    m_down(top).start()
                z_down(top, half).start()

        if half == 1:

            @pl.when(jnp.logical_and(low == 0, level + 1 < levels))
            def _():
                up_copy(kv, ep).start()

    def reach(k):
        low, top = level - k, level + k
        first = jnp.where(k <= both, 2 * k - 1, both + k)
        for half in range(2):
            pass_on(k, half)

            @pl.when(low >= 0)
            def _():
                hand_out(low, first, half)

            @pl.when(top < levels)
            def _():
                hand_out(top, jnp.where(k <= both, 2 * k, both + k), half)

            if half == 0:
                interior = jnp.logical_and(k > level, k <= 2 * level)

                @pl.when(jnp.logical_and(level + 1 < levels, interior))
                def _():
                    keys_on(k - level)

                @pl.when(k > 2)
                def _():
                    experts(k - 2)

            if half == 1:

                @pl.when(jnp.logical_and(level + 1 < levels, k == levels - 1))
                def _():
                    each(jnp.maximum(levels - level, 1), level + 1, keys_on)

                relay(k - 1)

                @pl.when(k == 1)
                def _():
                    for load in loads:
                        load.wait()

                @pl.when(jnp.logical_or(k == 1, k == levels - 1))
                def _():
                    experts(k - 1)

            @pl.when(jnp.logical_or(low >= 0, top < levels))
            def _():
                from_side(first, half)

            @pl.when(k <= both)
            def _():
                from_side(2 * k, half)

    each(1, levels, reach)

    @pl.when(side == 0)
    def _():
        side_copy(kv, ep).start()

    def send_both(number):
        send_back(number, 1 - side)
        send_back(number, side)

    def top_keys(begin, end):
        @pl.when(level + 1 == levels)
        def _():
            each(begin, end, keys_on)

    early = jnp.where(both == 1, 1, levels - 2)
    late = jnp.where(both == 1, levels - 2, 1)
    add(early)
    top_keys(1, levels // 2)
    relay(levels - 1)
    top_keys(levels // 2, 3 * levels // 4)
    experts(levels - 1)
    send_back(early, 1 - side)
    add(levels - 1)
    add(late)
    each(2, levels - 2, add)
    top_keys(3 * levels // 4, levels)
    send_back(early, side)
    each(1, level + 1, attend)
    far_first()
    each(1 - side, lax.div(level, 2) + 1, attend_beside)
    far_second()
    each(lax.div(level, 2) + 1, level + 1, attend_beside)
    for head in range(heads):
        span = pl.ds(head * rows, rows)
        result = (accum[span, :] / denom[span, :]).astype(jnp.bfloat16)
        for owner in range(n_tp):
            att[owner, head] = result[owner * part : (owner + 1) * part]
    for step in range(1, n_tp):
        t_copy(tp, step).start()
    att_all[tp] = att[tp]
    add(0)
    send_back(late, 1 - side)
    merge_on(0)
    send_back(late, side)
    merge_on(1)
    each(2, levels - 2, send_both)

    for step in range(1, n_tp):
        t_copy(lax.rem(tp - step + n_tp, n_tp), step).wait()
    chunk = min(width, 512)
    strips = [slice(begin, begin + chunk) for begin in range(0, width, chunk)]
    for lanes in strips:
        total = None
        for source in range(n_tp):
            for head in range(heads):
                number = source * heads + head
                term = jnp.dot(
                    att_all[source, head],
                    mixer[number * head_dim : (number + 1) * head_dim, lanes],
                    preferred_element_type=jnp.float32,
                )
                total = term if total is None else total + term
        mixed_v[:, lanes] = total.astype(jnp.bfloat16)
    mixed_out = pltpu.make_async_copy(mixed_v, mixed, o_sem.at[len(strips)])
    mixed_out.start()

    columns = meta[level].T
    slots = lax.broadcasted_iota(jnp.int32, (tokens, 2 * per), 1)
    for lower in range(levels):
        names = (lower * 2 * per + slots).astype(jnp.float32)
        for k in range(choices):
            picked[lower, k] = jnp.where(names == columns[:, k : k + 1], 1.0, 0.0).astype(
                jnp.bfloat16
            )
    weighing[...] = columns
    gathered[...] = jnp.zeros(gathered.shape, jnp.float32)

    def gather(source, lanes):
        found_rows = back[pl.ds(2 * source, 2), :, lanes].reshape(2 * per, chunk)
        summed = gathered[:, lanes]
        for k in range(choices):
            found = jnp.dot(picked[source, k], found_rows, preferred_element_type=jnp.float32)
            summed = summed + found * weighing[:, choices + k : choices + k + 1]
        return summed

    def far_rows(number):
        source = level_of(number)

        @pl.when(jnp.logical_not(jnp.logical_and(edge, number >= levels - 2)))
        def _():
            r_arrived(pair(back, source), source).wait_recv()
            for lanes in strips:
                gathered[:, lanes] = gather(source, lanes)

    send_back(0, 1 - side)
    each(1, levels, far_rows)

    @pl.when(edge)
    def _():
        remote(part_v, merged, g_send.at[0], h_recv.at[0], beside, tp).wait_recv()
        for lanes in strips:
            gathered[:, lanes] = gathered[:, lanes] + merged[:, lanes].astype(jnp.float32)

    for half in range(2):
        back[ep, :, halves[half]] = total_of(side, half)
    r_arrived(back.at[beside], level).wait_recv()
    outs = []
    for strip_number, lanes in enumerate(strips):
        routed_v[:, lanes] = gather(level, lanes).astype(jnp.bfloat16)
        out = pltpu.make_async_copy(routed_v.at[:, lanes], routed.at[:, lanes], o_sem.at[strip_number])
        out.start()
        outs.append(out)

    for move, whole in (
        (x_move, pieces.at[tp]),
        (c_move, pieces.at[tp]),
        (d_move, pieces.at[across]),
        (f_move, sums.at[corner]),
        (n_move, sums.at[core]),
    ):
        move(whole, whole, 0).wait_send()
    remote(sum_x, got_x, y_send.at[0], y_recv.at[0], ep, across).wait_send()

    def back_sent(count):
        most = pl.ds(0, count)
        remote(sum_r.at[most], back.at[most], r_send.at[0], r_recv.at[0], beside, tp).wait_send()

    @pl.when(joins)
    def _():
        back_sent(n_ep - 3)
        src, dst = sum_r.at[0], pair_rows.at[0]
        remote(src, dst, p_send.at[0], p_recv.at[0], beside, tp).wait_send()
        remote(part_v, merged, g_send.at[0], h_recv.at[0], beside, tp).wait_send()

    @pl.when(jnp.logical_not(joins))
    def _():
        back_sent(n_ep - 1)

    remote(ysend, ysend, b_send.at[0], b_recv.at[0], beside, tp).wait_send()

    def passed(source):
        @pl.when(jnp.logical_and(source <= level, level + 1 < levels))
        def _():
            m_up(source).wait_send()
            passed_all(source, zu_send).wait_send()

        @pl.when(jnp.logical_and(source >= level, level > 0))
        def _():
            m_down(source).wait_send()
            passed_all(source, zd_send).wait_send()

    each(0, levels, passed)

    @pl.when(level + 1 < levels)
    def _():
        up_copy(kv, ep).wait_send()

    @pl.when(side == 0)
    def _():
        side_copy(kv, ep).wait_send()

    def keys_sent(k):
        source = ep - 2 * k
        side_copy(kv, source).wait_send()

        @pl.when(level + 1 < levels)
        def _():
            up_copy(kv, source).wait_send()

    each(1, level + 1, keys_sent)

    def finish():
        mixed_out.wait()
        for out in outs:
            out.wait()

    finish()


def hand_off(mixed, routed, mixed_out, routed_out, mixed_v, routed_v, in_sem, out_sem):
    parts = 2
    moves = []
    for which, (src, held, dst) in enumerate(
        [(mixed, mixed_v, mixed_out), (routed, routed_v, routed_out)]
    ):
        lines = src.shape[0] // parts
        for number in range(parts):
            span = slice(number * lines, (number + 1) * lines)
            at = which * parts + number
            moves.append(
                (
                    pltpu.make_async_copy(src.at[span], held.at[span], in_sem.at[at]),
                    pltpu.make_async_copy(held.at[span], dst.at[span], out_sem.at[at]),
                )
            )
    for load, _ in moves:
        load.start()
    for load, store in moves:
        load.wait()
        store.start()
    for _, store in moves:
        store.wait()


def on_device(
    n_ep,
    n_tp,
    queries,
    keys,
    values,
    forget_cache,
    query_gain,
    key_gain,
    mixer_out,
    expert_input,
    norm_gain,
    routes,
    route_weights,
    w_gate,
    w_up,
    w_down,
):
    rows, head_dim = keys.shape
    heads = forget_cache.shape[0]
    local, width, ff = w_gate.shape
    tokens = expert_input.shape[0]
    per = local * CAP
    part = rows // n_tp
    levels = n_ep // 2
    vmem = pl.BlockSpec(memory_space=pltpu.VMEM)
    anywhere = pl.BlockSpec(memory_space=pl.ANY)
    dma = pltpu.SemaphoreType.DMA
    buffer = pltpu.VMEM((n_ep, per, width), jnp.bfloat16)
    mixed, routed = pl.pallas_call(
        functools.partial(layer_kernel, n_ep, n_tp),
        out_shape=(
            jax.ShapeDtypeStruct((part, width), jnp.bfloat16),
            jax.ShapeDtypeStruct((tokens, width), jnp.bfloat16),
        ),
        in_specs=[vmem] * 10 + [anywhere] * 4,
        out_specs=(anywhere, anywhere),
        scratch_shapes=[pltpu.VMEM(w_gate.shape, jnp.bfloat16)] * 3
        + [
            pltpu.VMEM(mixer_out.shape, jnp.bfloat16),
            pltpu.VMEM((rows, 2 * head_dim), jnp.bfloat16),
            pltpu.VMEM((n_ep, rows, 2 * head_dim), jnp.bfloat16),
            pltpu.VMEM((heads * rows, head_dim), jnp.bfloat16),
            pltpu.VMEM((heads * rows, head_dim), jnp.float32),
            pltpu.VMEM((levels, tokens, width), jnp.bfloat16),
            pltpu.VMEM((levels, 8, tokens), jnp.float32),
            pltpu.VMEM((levels, per, width), jnp.bfloat16),
            pltpu.VMEM((n_tp, heads, part, head_dim), jnp.bfloat16),
            pltpu.VMEM((n_tp, heads, part, head_dim), jnp.bfloat16),
            pltpu.VMEM((heads * rows, 1), jnp.float32),
            pltpu.VMEM((heads * rows, 1), jnp.float32),
            pltpu.VMEM((heads * rows, head_dim), jnp.float32),
            pltpu.VMEM((n_tp, n_ep, per, width), jnp.bfloat16),
            pltpu.VMEM((n_tp, n_ep, per, width), jnp.bfloat16),
        ]
        + [buffer] * 6
        + [dma((1,)), dma((levels,))] * 5
        + [dma((1,)), dma((2 * n_ep,)), dma((1,)), dma((levels,))]
        + [dma((levels,)), dma((levels,)), dma((n_ep,))]
        + [dma((levels,))] * 3
        + [dma((1,)), dma((n_ep,))]
        + [dma((levels,)), dma((levels,)), dma((n_ep,))]
        + [dma((n_tp,))] * 2
        + [
            dma((4,)),
            pltpu.VMEM((part, width), jnp.bfloat16),
            pltpu.VMEM((tokens, width), jnp.bfloat16),
            pltpu.VMEM((levels, routes.shape[1], tokens, 2 * per), jnp.bfloat16),
            pltpu.VMEM((tokens, 8), jnp.float32),
            pltpu.VMEM((tokens, width), jnp.float32),
            dma((width // min(width, 512) + 1,)),
            pltpu.VMEM((2, per, width), jnp.bfloat16),
        ]
        + [pltpu.VMEM((tokens, width), jnp.bfloat16)] * 3
        + [
            dma((1,)),
            dma((2,)),
            dma((1,)),
            dma((2,)),
            dma((1,)),
        ],
        compiler_params=pltpu.CompilerParams(
            collective_id=0, has_side_effects=True, vmem_limit_bytes=VMEM_LIMIT
        ),
        name="layer",
    )(
        expert_input,
        norm_gain.reshape(1, width),
        routes.T,
        route_weights.T,
        queries,
        keys,
        values,
        forget_cache,
        query_gain.reshape(1, head_dim),
        key_gain.reshape(1, head_dim),
        w_gate,
        w_up,
        w_down,
        mixer_out,
    )
    return pl.pallas_call(
        hand_off,
        out_shape=tuple(jax.ShapeDtypeStruct(part.shape, part.dtype) for part in (mixed, routed)),
        in_specs=[anywhere] * 2,
        out_specs=(anywhere, anywhere),
        scratch_shapes=[pltpu.VMEM(part.shape, part.dtype) for part in (mixed, routed)]
        + [dma((4,))] * 2,
        name="hand_off",
    )(mixed, routed)


def solution(mesh):
    n_ep, n_tp = mesh.shape["ep"], mesh.shape["tp"]
    in_specs = (
        P("ep", "tp"),
        P("ep", "tp"),
        P("ep", "tp"),
        P("tp", None),
        P(),
        P(),
        P(),
        P(("ep", "tp"), None),
        P(),
        P(("ep", "tp"), None),
        P(("ep", "tp"), None),
        P("ep", None, "tp"),
        P("ep", None, "tp"),
        P("ep", None, "tp"),
    )
    out_specs = (P(("ep", "tp"), None), P(("ep", "tp"), None))
    return jax.shard_map(
        functools.partial(on_device, n_ep, n_tp),
        mesh=mesh,
        in_specs=in_specs,
        out_specs=out_specs,
        check_vma=False,
    )
```

```python
import functools

import jax
import jax.numpy as jnp
from jax import lax
from jax.experimental import pallas as pl
from jax.experimental.pallas import tpu as pltpu
from jax.sharding import PartitionSpec as P

CAP = 16
EPSILON = 1e-06
NEGATIVE = -1e30
MESH = pl.DeviceIdType.MESH
VMEM_LIMIT = 63 * 1024 * 1024


def places(n_tp):
    ep, tp = lax.axis_index("ep"), lax.axis_index("tp")
    core = tp + 1 - 2 * lax.rem(tp, 2)
    across = lax.rem(tp + n_tp // 2, n_tp)
    corner = lax.rem(core + n_tp // 2, n_tp)
    return ep, tp, core, across, corner


def remote(src, dst, send, recv, ep, tp):
    return pltpu.make_async_remote_copy(
        src_ref=src, dst_ref=dst, send_sem=send, recv_sem=recv, device_id=(ep, tp), device_id_type=MESH
    )


def normed_rows(ref, columns, gain):
    values = ref[:, columns].astype(jnp.float32)
    inverse = lax.rsqrt(jnp.mean(values * values, axis=-1, keepdims=True) + EPSILON)
    return (values * inverse * gain).astype(jnp.bfloat16)


def layer_kernel(
    n_ep,
    n_tp,
    tokens_in,
    norm_gain,
    routes,
    route_weights,
    queries,
    keys_in,
    values_in,
    forget,
    query_gain,
    key_gain,
    gate_hbm,
    up_hbm,
    down_hbm,
    mixer_hbm,
    mixed,
    routed,
    gate_w,
    up_w,
    down_w,
    mixer,
    kv,
    kvbuf,
    q,
    fq,
    tok,
    meta,
    ysend,
    att,
    att_all,
    high,
    denom,
    accum,
    pieces,
    sums,
    near_own,
    near_far,
    sum_x,
    got_x,
    sum_r,
    back,
    x_send,
    x_recv,
    c_send,
    c_recv,
    d_send,
    d_recv,
    f_send,
    f_recv,
    n_send,
    n_recv,
    y_send,
    y_recv,
    r_send,
    r_recv,
    zu_send,
    zd_send,
    z_recv,
    mu_send,
    md_send,
    m_recv,
    b_send,
    b_recv,
    u_send,
    k_send,
    k_recv,
    t_send,
    t_recv,
    w_sem,
    mixed_v,
    routed_v,
    picked,
    weighing,
    gathered,
    o_sem,
    pair_rows,
    part_v,
    far_in,
    merged,
    p_send,
    p_recv,
    g_send,
    g_recv,
    h_recv,
):
    ep, tp, core, across, corner = places(n_tp)
    rows, head_dim = keys_in.shape
    heads = forget.shape[0]
    part = rows // n_tp
    scale = head_dim ** (-0.5)
    local, width, ff = gate_w.shape
    per = local * CAP
    tokens = tokens_in.shape[0]
    choices = routes.shape[0]
    level, side = lax.div(ep, 2), lax.rem(ep, 2)
    levels = n_ep // 2
    beside = ep + 1 - 2 * side
    above = lax.rem(ep + 2, n_ep)
    below = lax.rem(ep + n_ep - 2, n_ep)
    both = jnp.minimum(level, levels - 1 - level)
    edge, joins = both == 0, both <= 1
    assert levels >= 4
    halves = [slice(0, width // 2), slice(width // 2, width)]

    loads = [
        pltpu.make_async_copy(src, dst, w_sem.at[number])
        for number, (src, dst) in enumerate(
            [(gate_hbm, gate_w), (up_hbm, up_w), (down_hbm, down_w), (mixer_hbm, mixer)]
        )
    ]
    for load in loads:
        load.start()

    barrier = pltpu.get_barrier_semaphore()
    for step in range(1, n_ep):
        pl.semaphore_signal(
            barrier, inc=1, device_id=(lax.rem(ep + step, n_ep), tp), device_id_type=MESH
        )
    for step in range(1, n_tp):
        pl.semaphore_signal(
            barrier, inc=1, device_id=(ep, lax.rem(tp + step, n_tp)), device_id_type=MESH
        )

    def each(first, last, act):
        def body(number, carry):
            act(number)
            return carry

        lax.fori_loop(first, last, body, 0)

    def level_of(number):
        near = lax.div(number + 1, 2)
        odd = lax.rem(number, 2)
        far = number - both
        paired = level + near * (1 - 2 * odd)
        lone = jnp.where(level < levels - 1 - level, level + far, level - far)
        return jnp.where(number <= 2 * both, paired, lone)

    def z_up(source, half):
        lines = tok.at[source, :, halves[half]]
        return remote(lines, lines, zu_send.at[source], z_recv.at[2 * source + half], above, tp)

    def z_down(source, half):
        lines = tok.at[source, :, halves[half]]
        return remote(lines, lines, zd_send.at[source], z_recv.at[2 * source + half], below, tp)

    def passed_all(source, sems):
        block = tok.at[source]
        return remote(block, block, sems.at[source], z_recv.at[0], above, tp)

    def m_up(source):
        return remote(meta.at[source], meta.at[source], mu_send.at[source], m_recv.at[source], above, tp)

    def m_down(source):
        return remote(meta.at[source], meta.at[source], md_send.at[source], m_recv.at[source], below, tp)

    def b_copy(number, half):
        slot = 2 * number + side
        piece = 2 * number + half
        return remote(
            ysend.at[number, :, halves[half]],
            pieces.at[tp, slot, :, halves[half]],
            b_send.at[0],
            b_recv.at[piece],
            beside,
            tp,
        )

    def up_copy(src, source):
        return remote(src, kvbuf.at[source], u_send.at[lax.div(source, 2)], k_recv.at[source], above, tp)

    def side_copy(src, source):
        return remote(src, kvbuf.at[source], k_send.at[lax.div(source, 2)], k_recv.at[source], beside, tp)

    def x_move(src, dst, slot):
        return remote(src, dst, x_send.at[0], x_recv.at[lax.div(slot, 2)], ep, across)

    def c_move(src, dst, slot):
        return remote(src, dst, c_send.at[0], c_recv.at[lax.div(slot, 2)], ep, core)

    def d_move(src, dst, slot):
        return remote(src, dst, d_send.at[0], d_recv.at[lax.div(slot, 2)], ep, core)

    def f_move(src, dst, slot):
        return remote(src, dst, f_send.at[0], f_recv.at[lax.div(slot, 2)], ep, core)

    def n_move(src, dst, slot):
        return remote(src, dst, n_send.at[0], n_recv.at[lax.div(slot, 2)], ep, core)

    def x_copy(slot, lanes):
        piece = pieces.at[tp, slot, :, lanes]
        return x_move(piece, piece, slot)

    def c_copy(slot, lanes):
        piece = pieces.at[tp, slot, :, lanes]
        return c_move(piece, piece, slot)

    def d_copy(slot):
        piece = pieces.at[across, slot]
        return d_move(piece, piece, slot)

    def far_copy(slot):
        return f_move(sums.at[corner, slot], near_far.at[slot], slot)

    def own_copy(slot):
        return n_move(sums.at[core, slot], near_own.at[slot], slot)

    def pair(buffer, number):
        return buffer.at[pl.ds(2 * number, 2)]

    def y_copy(slot, half):
        lanes, piece = halves[half], 2 * slot + half
        return remote(
            sum_x.at[slot, :, lanes],
            got_x.at[slot, :, lanes],
            y_send.at[0],
            y_recv.at[piece],
            ep,
            across,
        )

    def r_copy(slot, dest, lanes=slice(None)):
        src, dst = sum_r.at[slot, :, lanes], back.at[ep, :, lanes]
        return remote(src, dst, r_send.at[0], r_recv.at[level], dest, tp)

    def r_arrived(rows_of, source):
        return remote(rows_of, rows_of, r_send.at[0], r_recv.at[source], beside, tp)

    def t_copy(source, step):
        dest = lax.rem(tp + step, n_tp)
        return remote(att.at[dest], att_all.at[source], t_send.at[step], t_recv.at[source], ep, dest)

    strip = min(tokens, 32)
    for begin in range(0, tokens, strip):
        lines = slice(begin, begin + strip)
        values = tokens_in[lines, :].astype(jnp.float32)
        inverse = lax.rsqrt(jnp.mean(values * values, axis=-1, keepdims=True) + EPSILON)
        tok[level, lines, :] = (values * inverse * norm_gain[...]).astype(jnp.bfloat16)
    names = lax.broadcasted_iota(jnp.int32, (n_ep * local, tokens), 0)
    named = [names == routes[k : k + 1, :] for k in range(choices)]
    anyone = sum(jnp.where(mine, 1.0, 0.0) for mine in named).astype(jnp.bfloat16)
    earlier = jnp.where(
        lax.broadcasted_iota(jnp.int32, (tokens, tokens), 0)
        < lax.broadcasted_iota(jnp.int32, (tokens, tokens), 1),
        1.0,
        0.0,
    ).astype(jnp.bfloat16)
    prior = jnp.dot(anyone, earlier, preferred_element_type=jnp.float32)
    meta[level] = jnp.zeros(meta.shape[1:], jnp.float32)
    for k in range(choices):
        rank = jnp.sum(jnp.where(named[k], prior, 0.0), axis=0, keepdims=True)
        meta[level, k : k + 1, :] = routes[k : k + 1, :].astype(jnp.float32) * CAP + rank
    meta[level, choices : 2 * choices, :] = route_weights[...]

    def select(source, place, lanes):
        lines = place * per + lax.broadcasted_iota(jnp.int32, (per, tokens), 0)
        lines = lines.astype(jnp.float32)
        picks = functools.reduce(
            jnp.logical_or, [lines == meta[source, k : k + 1, :] for k in range(choices)]
        )
        picks = jnp.where(picks, 1.0, 0.0).astype(jnp.bfloat16)
        found = jnp.dot(picks, tok[source, :, lanes], preferred_element_type=jnp.float32)
        return found.astype(jnp.bfloat16)

    def pick_rows(source, number, half):
        lanes = halves[half]
        pieces[tp, 2 * number + side, :, lanes] = select(source, ep, lanes)
        ysend[number, :, lanes] = select(source, beside, lanes)

    def send_rows(number, half):
        slot = 2 * number + side
        x_copy(slot, halves[half]).start()
        b_copy(number, half).start()
        c_copy(slot, halves[half]).start()

    for half in range(2):
        pick_rows(level, 0, half)

    pl.semaphore_wait(barrier, n_ep + n_tp - 2)
    for half in range(2):
        send_rows(0, half)

    @pl.when(level + 1 < levels)
    def _():
        m_up(level).start()
        for half in range(2):
            z_up(level, half).start()

    @pl.when(level > 0)
    def _():
        m_down(level).start()
        for half in range(2):
            z_down(level, half).start()

    def hand_out(source, number, half):
        pick_rows(source, number, half)
        send_rows(number, half)

    def from_side(number, half):
        slot = 2 * number + 1 - side
        b_copy(number, half).wait_recv()
        x_copy(slot, halves[half]).start()
        c_copy(slot, halves[half]).start()

    def relay(number):
        whole = pair(pieces.at[across], number)
        x_move(whole, whole, 2 * number).wait_recv()
        for slot in (2 * number, 2 * number + 1):
            d_copy(slot).start()

    def expert(number, begin):
        own_rows = pl.ds(pl.multiple_of(number * CAP, CAP), CAP)
        taken = pieces[:, pl.ds(begin, 2), own_rows, :].reshape(n_tp * 2 * CAP, width)
        gate = jnp.dot(taken, gate_w[number], preferred_element_type=jnp.float32)
        upward = jnp.dot(taken, up_w[number], preferred_element_type=jnp.float32)
        hidden = (gate / (1.0 + jnp.exp(-gate)) * upward).astype(jnp.bfloat16)
        columns = min(width, 512)
        for begin_column in range(0, width, columns):
            lanes = slice(begin_column, begin_column + columns)
            result = lax.dot_general(
                hidden,
                down_w[number, lanes, :],
                (((1,), (1,)), ((), ())),
                preferred_element_type=jnp.float32,
            )
            sums[:, pl.ds(begin, 2), own_rows, lanes] = result.astype(jnp.bfloat16).reshape(
                n_tp, 2, CAP, columns
            )

    def experts(number):
        whole = pair(pieces.at[core], number)
        c_move(whole, whole, 2 * number).wait_recv()
        d_move(whole, whole, 2 * number).wait_recv()
        each(0, local, lambda which: expert(which, 2 * number))
        for slot in (2 * number, 2 * number + 1):
            far_copy(slot).start()
            own_copy(slot).start()

    def add(number):
        whole = pair(near_far, number)
        f_move(whole, whole, 2 * number).wait_recv()
        for other in (1 - side, side):
            slot = 2 * number + other
            for half in range(2):
                lanes = halves[half]
                sum_x[slot, :, lanes] = (
                    sums[across, slot, :, lanes].astype(jnp.float32)
                    + near_far[slot, :, lanes].astype(jnp.float32)
                ).astype(jnp.bfloat16)
                y_copy(slot, half).start()

    def own_landed(number, other):
        @pl.when(other != side)
        def _():
            whole = pair(near_own, number)
            n_move(whole, whole, 2 * number).wait_recv()

    def total_of(slot, half):
        lanes = halves[half]
        y_copy(slot, half).wait_recv()
        return (
            sums[tp, slot, :, lanes].astype(jnp.float32)
            + near_own[slot, :, lanes].astype(jnp.float32)
            + got_x[slot, :, lanes].astype(jnp.float32)
        ).astype(jnp.bfloat16)

    def send_back(number, other):
        slot = 2 * number + other
        own_landed(number, other)
        for half in range(2):
            sum_r[slot, :, halves[half]] = total_of(slot, half)
            r_copy(slot, 2 * level_of(number) + other, halves[half]).start()

    goal = level_of(levels - 1)
    toward = jnp.where(level == 0, above, below)

    def p_copy(half):
        src = sum_r.at[2 * levels - 1 - side, :, halves[half]]
        dst = pair_rows.at[side, :, halves[half]]
        return remote(src, dst, p_send.at[0], p_recv.at[half], beside, tp)

    def g_copy(half):
        src, dst = part_v.at[:, halves[half]], far_in.at[:, halves[half]]
        return remote(src, dst, g_send.at[0], g_recv.at[half], toward, tp)

    def h_copy(half):
        src, dst = part_v.at[:, halves[half]], merged.at[:, halves[half]]
        return remote(src, dst, g_send.at[0], h_recv.at[0], 2 * goal + side, tp)

    def weighed(half):
        p_copy(half).wait_recv()
        columns = meta[goal].T
        names = 2 * per * level + lax.broadcasted_iota(jnp.int32, (tokens, 2 * per), 1)
        names = names.astype(jnp.float32)
        rows_of = pair_rows[:, :, halves[half]].reshape(2 * per, width // 2)
        summed = None
        for k in range(choices):
            pick = jnp.where(names == columns[:, k : k + 1], 1.0, 0.0).astype(jnp.bfloat16)
            found = jnp.dot(pick, rows_of, preferred_element_type=jnp.float32)
            term = found * columns[:, choices + k : choices + k + 1]
            summed = term if summed is None else summed + term
        return summed

    def merge_out(half):
        part_v[:, halves[half]] = weighed(half).astype(jnp.bfloat16)
        g_copy(half).start()

    def merge_on(half):
        @pl.when(jnp.logical_and(joins, jnp.logical_not(edge)))
        def _():
            summed = weighed(half)
            g_copy(half).wait_recv()
            summed = summed + far_in[:, halves[half]].astype(jnp.float32)
            part_v[:, halves[half]] = summed.astype(jnp.bfloat16)
            h_copy(half).start()

    def far_first():
        @pl.when(joins)
        def _():
            slot = 2 * levels - 1 - side
            own_landed(levels - 1, 1 - side)
            for half in range(2):
                sum_r[slot, :, halves[half]] = total_of(slot, half)
                p_copy(half).start()

        @pl.when(jnp.logical_not(joins))
        def _():
            send_back(levels - 1, 1 - side)

    def far_second():
        @pl.when(joins)
        def _():
            for half in range(2):
                pair_rows[side, :, halves[half]] = total_of(2 * levels - 2 + side, half)

        @pl.when(jnp.logical_not(joins))
        def _():
            send_back(levels - 1, side)

        @pl.when(edge)
        def _():
            for half in range(2):
                merge_out(half)

    tile = rows // 2

    def block(source, keys_ref, diagonal):
        keys = keys_ref[:, :head_dim]
        vals = keys_ref[:, head_dim:]
        at = pl.ds(pl.multiple_of(source * rows, rows), rows)
        for head in range(heads):
            key_gate = forget[head : head + 1, at]
            for piece in range(2):
                span = pl.ds(head * rows + piece * tile, tile)
                scores = lax.dot_general(
                    q[span, :], keys, (((1,), (1,)), ((), ())), preferred_element_type=jnp.float32
                )
                scores = scores * scale + fq[span, 0:1] - key_gate
                if diagonal:
                    qpos = piece * tile + lax.broadcasted_iota(jnp.int32, scores.shape, 0)
                    kpos = lax.broadcasted_iota(jnp.int32, scores.shape, 1)
                    scores = jnp.where(kpos <= qpos, scores, NEGATIVE)
                top = jnp.max(scores, axis=1, keepdims=True)
                if diagonal:
                    newest = top
                else:
                    before = high[span, :]
                    newest = jnp.maximum(before, top)
                weights = jnp.exp(scores - newest)
                total = jnp.sum(weights, axis=1, keepdims=True)
                product = jnp.dot(
                    weights.astype(jnp.bfloat16), vals, preferred_element_type=jnp.float32
                )
                if not diagonal:
                    factor = jnp.exp(before - newest)
                    total = denom[span, :] * factor + total
                    product = accum[span, :] * factor + product
                high[span, :] = newest
                denom[span, :] = total
                accum[span, :] = product

    def keys_on(k):
        lower = ep - 2 * k
        side_copy(kv, lower).wait_recv()
        side_copy(kvbuf.at[lower], lower).start()

        @pl.when(level + 1 < levels)
        def _():
            up_copy(kvbuf.at[lower], lower).start()

    def attend(k):
        lower = ep - 2 * k
        block(lower, kvbuf.at[lower], False)

    def attend_beside(k):
        other = 2 * (level - k) + 1 - side
        side_copy(kv, other).wait_recv()
        block(other, kvbuf.at[other], False)


    kv[:, :head_dim] = normed_rows(keys_in, slice(None), key_gain[...])
    kv[:, head_dim:] = values_in[...]

    @pl.when(level == 0)
    def _():
        up_copy(kv, ep).start()

    mine = pl.ds(pl.multiple_of(ep * rows, rows), rows)
    for head in range(heads):
        lines = slice(head * rows, (head + 1) * rows)
        lanes = slice(head * head_dim, (head + 1) * head_dim)
        q[lines, :] = normed_rows(queries, lanes, query_gain[...])
        fq[lines, :] = jnp.broadcast_to(forget[head : head + 1, mine], (head_dim, rows)).T

    for half in range(2):
        from_side(0, half)
    block(ep, kv, True)

    def pass_on(k, half):
        low, top = level - k, level + k

        @pl.when(low >= 0)
        def _():
            if half == 0:
                m_up(low).wait_recv()
            z_up(low, half).wait_recv()

            @pl.when(level + 1 < levels)
            def _():
                if half == 0:
                    m_up(low).start()
                z_up(low, half).start()

        @pl.when(top < levels)
        def _():
            if half == 0:
                m_down(top).wait_recv()
            z_down(top, half).wait_recv()

            @pl.when(level > 0)
            def _():
                if half == 0:
                    m_down(top).start()
                z_down(top, half).start()

        if half == 1:

            @pl.when(jnp.logical_and(low == 0, level + 1 < levels))
            def _():
                up_copy(kv, ep).start()

    def reach(k):
        low, top = level - k, level + k
        first = jnp.where(k <= both, 2 * k - 1, both + k)
        for half in range(2):
            pass_on(k, half)

            @pl.when(low >= 0)
            def _():
                hand_out(low, first, half)

            @pl.when(top < levels)
            def _():
                hand_out(top, jnp.where(k <= both, 2 * k, both + k), half)

            if half == 0:
                interior = jnp.logical_and(k > level, k <= 2 * level)

                @pl.when(jnp.logical_and(level + 1 < levels, interior))
                def _():
                    keys_on(k - level)

                @pl.when(k > 2)
                def _():
                    experts(k - 2)

            if half == 1:

                @pl.when(jnp.logical_and(level + 1 < levels, k == levels - 1))
                def _():
                    each(jnp.maximum(levels - level, 1), level + 1, keys_on)

                relay(k - 1)

                @pl.when(k == 1)
                def _():
                    for load in loads:
                        load.wait()

                @pl.when(jnp.logical_or(k == 1, k == levels - 1))
                def _():
                    experts(k - 1)

            @pl.when(jnp.logical_or(low >= 0, top < levels))
            def _():
                from_side(first, half)

            @pl.when(k <= both)
            def _():
                from_side(2 * k, half)

    each(1, levels, reach)

    @pl.when(side == 0)
    def _():
        side_copy(kv, ep).start()

    def send_both(number):
        send_back(number, 1 - side)
        send_back(number, side)

    def top_keys(begin, end):
        @pl.when(level + 1 == levels)
        def _():
            each(begin, end, keys_on)

    early = jnp.where(both == 1, 1, levels - 2)
    late = jnp.where(both == 1, levels - 2, 1)
    add(early)
    top_keys(1, levels // 2)
    relay(levels - 1)
    top_keys(levels // 2, 3 * levels // 4)
    experts(levels - 1)
    send_back(early, 1 - side)
    add(levels - 1)
    add(late)
    each(2, levels - 2, add)
    top_keys(3 * levels // 4, levels)
    send_back(early, side)
    each(1, level + 1, attend)
    far_first()
    each(1 - side, lax.div(level, 2) + 1, attend_beside)
    far_second()
    each(lax.div(level, 2) + 1, level + 1, attend_beside)
    for head in range(heads):
        span = pl.ds(head * rows, rows)
        result = (accum[span, :] / denom[span, :]).astype(jnp.bfloat16)
        for owner in range(n_tp):
            att[owner, head] = result[owner * part : (owner + 1) * part]
    for step in range(1, n_tp):
        t_copy(tp, step).start()
    att_all[tp] = att[tp]
    add(0)
    send_back(late, 1 - side)
    merge_on(0)
    send_back(late, side)
    merge_on(1)
    each(2, levels - 2, send_both)

    for step in range(1, n_tp):
        t_copy(lax.rem(tp - step + n_tp, n_tp), step).wait()
    chunk = min(width, 512)
    strips = [slice(begin, begin + chunk) for begin in range(0, width, chunk)]
    for lanes in strips:
        total = None
        for source in range(n_tp):
            for head in range(heads):
                number = source * heads + head
                term = jnp.dot(
                    att_all[source, head],
                    mixer[number * head_dim : (number + 1) * head_dim, lanes],
                    preferred_element_type=jnp.float32,
                )
                total = term if total is None else total + term
        mixed_v[:, lanes] = total.astype(jnp.bfloat16)
    mixed_out = pltpu.make_async_copy(mixed_v, mixed, o_sem.at[len(strips)])
    mixed_out.start()

    columns = meta[level].T
    slots = lax.broadcasted_iota(jnp.int32, (tokens, 2 * per), 1)
    for lower in range(levels):
        names = (lower * 2 * per + slots).astype(jnp.float32)
        for k in range(choices):
            picked[lower, k] = jnp.where(names == columns[:, k : k + 1], 1.0, 0.0).astype(
                jnp.bfloat16
            )
    weighing[...] = columns
    gathered[...] = jnp.zeros(gathered.shape, jnp.float32)

    def gather(source, lanes):
        found_rows = back[pl.ds(2 * source, 2), :, lanes].reshape(2 * per, chunk)
        summed = gathered[:, lanes]
        for k in range(choices):
            found = jnp.dot(picked[source, k], found_rows, preferred_element_type=jnp.float32)
            summed = summed + found * weighing[:, choices + k : choices + k + 1]
        return summed

    def far_rows(number):
        source = level_of(number)

        @pl.when(jnp.logical_not(jnp.logical_and(edge, number >= levels - 2)))
        def _():
            r_arrived(pair(back, source), source).wait_recv()
            for lanes in strips:
                gathered[:, lanes] = gather(source, lanes)

    send_back(0, 1 - side)
    each(1, levels, far_rows)

    @pl.when(edge)
    def _():
        remote(part_v, merged, g_send.at[0], h_recv.at[0], beside, tp).wait_recv()
        for lanes in strips:
            gathered[:, lanes] = gathered[:, lanes] + merged[:, lanes].astype(jnp.float32)

    r_arrived(back.at[beside], level).wait_recv()
    outs = []
    for half in range(2):
        back[ep, :, halves[half]] = total_of(side, half)
        for strip_number, lanes in enumerate(strips):
            if lanes.start // (width // 2) != half:
                continue
            routed_v[:, lanes] = gather(level, lanes).astype(jnp.bfloat16)
            out = pltpu.make_async_copy(
                routed_v.at[:, lanes], routed.at[:, lanes], o_sem.at[strip_number]
            )
            out.start()
            outs.append(out)

    for move, whole in (
        (x_move, pieces.at[tp]),
        (c_move, pieces.at[tp]),
        (d_move, pieces.at[across]),
        (f_move, sums.at[corner]),
        (n_move, sums.at[core]),
    ):
        move(whole, whole, 0).wait_send()
    remote(sum_x, got_x, y_send.at[0], y_recv.at[0], ep, across).wait_send()

    def back_sent(count):
        most = pl.ds(0, count)
        remote(sum_r.at[most], back.at[most], r_send.at[0], r_recv.at[0], beside, tp).wait_send()

    @pl.when(joins)
    def _():
        back_sent(n_ep - 3)
        src, dst = sum_r.at[0], pair_rows.at[0]
        remote(src, dst, p_send.at[0], p_recv.at[0], beside, tp).wait_send()
        remote(part_v, merged, g_send.at[0], h_recv.at[0], beside, tp).wait_send()

    @pl.when(jnp.logical_not(joins))
    def _():
        back_sent(n_ep - 1)

    remote(ysend, ysend, b_send.at[0], b_recv.at[0], beside, tp).wait_send()

    def passed(source):
        @pl.when(jnp.logical_and(source <= level, level + 1 < levels))
        def _():
            m_up(source).wait_send()
            passed_all(source, zu_send).wait_send()

        @pl.when(jnp.logical_and(source >= level, level > 0))
        def _():
            m_down(source).wait_send()
            passed_all(source, zd_send).wait_send()

    each(0, levels, passed)

    @pl.when(level + 1 < levels)
    def _():
        up_copy(kv, ep).wait_send()

    @pl.when(side == 0)
    def _():
        side_copy(kv, ep).wait_send()

    def keys_sent(k):
        source = ep - 2 * k
        side_copy(kv, source).wait_send()

        @pl.when(level + 1 < levels)
        def _():
            up_copy(kv, source).wait_send()

    each(1, level + 1, keys_sent)

    def finish():
        mixed_out.wait()
        for out in outs:
            out.wait()

    finish()


def hand_off(mixed, routed, mixed_out, routed_out, mixed_v, routed_v, in_sem, out_sem):
    parts = 2
    moves = []
    for which, (src, held, dst) in enumerate(
        [(mixed, mixed_v, mixed_out), (routed, routed_v, routed_out)]
    ):
        lines = src.shape[0] // parts
        for number in range(parts):
            span = slice(number * lines, (number + 1) * lines)
            at = which * parts + number
            moves.append(
                (
                    pltpu.make_async_copy(src.at[span], held.at[span], in_sem.at[at]),
                    pltpu.make_async_copy(held.at[span], dst.at[span], out_sem.at[at]),
                )
            )
    for load, _ in moves:
        load.start()
    for load, store in moves:
        load.wait()
        store.start()
    for _, store in moves:
        store.wait()


def on_device(
    n_ep,
    n_tp,
    queries,
    keys,
    values,
    forget_cache,
    query_gain,
    key_gain,
    mixer_out,
    expert_input,
    norm_gain,
    routes,
    route_weights,
    w_gate,
    w_up,
    w_down,
):
    rows, head_dim = keys.shape
    heads = forget_cache.shape[0]
    local, width, ff = w_gate.shape
    tokens = expert_input.shape[0]
    per = local * CAP
    part = rows // n_tp
    levels = n_ep // 2
    vmem = pl.BlockSpec(memory_space=pltpu.VMEM)
    anywhere = pl.BlockSpec(memory_space=pl.ANY)
    dma = pltpu.SemaphoreType.DMA
    buffer = pltpu.VMEM((n_ep, per, width), jnp.bfloat16)
    mixed, routed = pl.pallas_call(
        functools.partial(layer_kernel, n_ep, n_tp),
        out_shape=(
            jax.ShapeDtypeStruct((part, width), jnp.bfloat16),
            jax.ShapeDtypeStruct((tokens, width), jnp.bfloat16),
        ),
        in_specs=[vmem] * 10 + [anywhere] * 4,
        out_specs=(anywhere, anywhere),
        scratch_shapes=[pltpu.VMEM(w_gate.shape, jnp.bfloat16)] * 3
        + [
            pltpu.VMEM(mixer_out.shape, jnp.bfloat16),
            pltpu.VMEM((rows, 2 * head_dim), jnp.bfloat16),
            pltpu.VMEM((n_ep, rows, 2 * head_dim), jnp.bfloat16),
            pltpu.VMEM((heads * rows, head_dim), jnp.bfloat16),
            pltpu.VMEM((heads * rows, head_dim), jnp.float32),
            pltpu.VMEM((levels, tokens, width), jnp.bfloat16),
            pltpu.VMEM((levels, 8, tokens), jnp.float32),
            pltpu.VMEM((levels, per, width), jnp.bfloat16),
            pltpu.VMEM((n_tp, heads, part, head_dim), jnp.bfloat16),
            pltpu.VMEM((n_tp, heads, part, head_dim), jnp.bfloat16),
            pltpu.VMEM((heads * rows, 1), jnp.float32),
            pltpu.VMEM((heads * rows, 1), jnp.float32),
            pltpu.VMEM((heads * rows, head_dim), jnp.float32),
            pltpu.VMEM((n_tp, n_ep, per, width), jnp.bfloat16),
            pltpu.VMEM((n_tp, n_ep, per, width), jnp.bfloat16),
        ]
        + [buffer] * 6
        + [dma((1,)), dma((levels,))] * 5
        + [dma((1,)), dma((2 * n_ep,)), dma((1,)), dma((levels,))]
        + [dma((levels,)), dma((levels,)), dma((n_ep,))]
        + [dma((levels,))] * 3
        + [dma((1,)), dma((n_ep,))]
        + [dma((levels,)), dma((levels,)), dma((n_ep,))]
        + [dma((n_tp,))] * 2
        + [
            dma((4,)),
            pltpu.VMEM((part, width), jnp.bfloat16),
            pltpu.VMEM((tokens, width), jnp.bfloat16),
            pltpu.VMEM((levels, routes.shape[1], tokens, 2 * per), jnp.bfloat16),
            pltpu.VMEM((tokens, 8), jnp.float32),
            pltpu.VMEM((tokens, width), jnp.float32),
            dma((width // min(width, 512) + 1,)),
            pltpu.VMEM((2, per, width), jnp.bfloat16),
        ]
        + [pltpu.VMEM((tokens, width), jnp.bfloat16)] * 3
        + [
            dma((1,)),
            dma((2,)),
            dma((1,)),
            dma((2,)),
            dma((1,)),
        ],
        compiler_params=pltpu.CompilerParams(
            collective_id=0, has_side_effects=True, vmem_limit_bytes=VMEM_LIMIT
        ),
        name="layer",
    )(
        expert_input,
        norm_gain.reshape(1, width),
        routes.T,
        route_weights.T,
        queries,
        keys,
        values,
        forget_cache,
        query_gain.reshape(1, head_dim),
        key_gain.reshape(1, head_dim),
        w_gate,
        w_up,
        w_down,
        mixer_out,
    )
    return pl.pallas_call(
        hand_off,
        out_shape=tuple(jax.ShapeDtypeStruct(part.shape, part.dtype) for part in (mixed, routed)),
        in_specs=[anywhere] * 2,
        out_specs=(anywhere, anywhere),
        scratch_shapes=[pltpu.VMEM(part.shape, part.dtype) for part in (mixed, routed)]
        + [dma((4,))] * 2,
        name="hand_off",
    )(mixed, routed)


def solution(mesh):
    n_ep, n_tp = mesh.shape["ep"], mesh.shape["tp"]
    in_specs = (
        P("ep", "tp"),
        P("ep", "tp"),
        P("ep", "tp"),
        P("tp", None),
        P(),
        P(),
        P(),
        P(("ep", "tp"), None),
        P(),
        P(("ep", "tp"), None),
        P(("ep", "tp"), None),
        P("ep", None, "tp"),
        P("ep", None, "tp"),
        P("ep", None, "tp"),
    )
    out_specs = (P(("ep", "tp"), None), P(("ep", "tp"), None))
    return jax.shard_map(
        functools.partial(on_device, n_ep, n_tp),
        mesh=mesh,
        in_specs=in_specs,
        out_specs=out_specs,
        check_vma=False,
    )
```
